256 devices in a mesh: ep: 32 (over z, x), tp: 8 (over y, core).
Axes of the slice: x: 4, y: 4, z: 8, core: 2. Of those that a mesh axis runs over, the one named last changes fastest.
Arguments:
- queries: bfloat16 [16384, 1024], P('ep', 'tp'), may hold values from -8 to 8
- keys_values: bfloat16 [16384, 1024], P('ep', 'tp'), may hold values from -60 to 60
- forget_cache: float32 [16, 16384], P('tp'), may hold values from -2460 to 0, as said below
- heads_gain: float32 [1024], replicated, may hold values from 0.1 to 1.9
- output_weight: bfloat16 [1024, 2048], replicated, may hold values from -0.1875 to 0.1875
- expert_tokens: bfloat16 [4096, 2048], P('ep'), may hold values from -600 to 600
- expert_gain: float32 [2048], replicated, may hold values from 0.1 to 1.9
- routes: int32 [4096, 4], P('ep'), may hold values from 0 to 31, all different within a row; in each aligned block of 128 rows (0 to 127, 128 to 255, ...) at most 32 rows name the same one
- route_logits: float32 [4096, 4], P('ep'), may hold values from -6 to 301
- gate_weight: bfloat16 [32, 2048, 2048], P('ep', None, 'tp'), may hold values from -0.5 to 0.5
- up_weight: bfloat16 [32, 2048, 2048], P('ep', None, 'tp'), may hold values from -0.5 to 0.5
- down_weight: bfloat16 [32, 2048, 2048], P('ep', 'tp'), may hold values from -0.015625 to 0.015625
Outputs:
- mixer_out: bfloat16 [16384, 2048], P(('ep', 'tp'))
- moe_out: bfloat16 [4096, 2048], P('ep', 'tp')
The draws below stay inside these ranges and needn't reach their ends.
Inputs may be any that keep to these rules, and one draw needn't show every extreme that they name: `forget_cache`: each row never rises from one position to the next. `routes`: the 4 experts of a row differ. In each aligned block of 128 rows (one device's tokens) no expert is named more than 32 times, so slot is below 32; some expert is named exactly 32 times in some block.
All inputs are finite; a program needn't handle non-finite values.
Results may differ from the reference program's by a relative error of at most 0.017.
Values may be sent and summed in bfloat16 or wider, within the bound.
A program may use at most 128 MiB of HBM per device.

```python
import math
import jax
import jax.numpy as jnp
import numpy as np
from jax import lax

D = 2048
ASKER_HEAD_TOTAL = 16
KV_HEADS = 8
HEAD = 64
FF = 2048
TOPK = 4
ATT_ROWS = 512
EXP_ROWS = 128
EXPERTS = 32
CAP = 32
MIXER_SEQ_SPAN = 16384
TOK_EXP = 4096
N_EP = 32
N_TP = 8


def base_values(key, shape):
    return jax.random.truncated_normal(key, -6.0, 6.0, shape, jnp.float32)


def draw_queries(key, part):
    result = base_values(jax.random.fold_in(key, 1), (MIXER_SEQ_SPAN, ASKER_HEAD_TOTAL, HEAD))
    return result.reshape(MIXER_SEQ_SPAN, ASKER_HEAD_TOTAL * HEAD).astype(jnp.bfloat16)


def draw_keys_values(key, part):
    key_rows = base_values(jax.random.fold_in(key, 2), (MIXER_SEQ_SPAN, KV_HEADS, HEAD))
    value_rows = base_values(jax.random.fold_in(key, 3), (MIXER_SEQ_SPAN, KV_HEADS, HEAD))
    scale_top = math.log(10.0)
    spread = jnp.exp(jax.random.uniform(jax.random.fold_in(key, 4), (1, KV_HEADS, HEAD), jnp.float32, 0.0, scale_top))
    value_rows = value_rows * spread
    joined = jnp.concatenate([key_rows, value_rows], axis=2)
    return joined.reshape(MIXER_SEQ_SPAN, KV_HEADS * 2 * HEAD).astype(jnp.bfloat16)


def draw_forget_cache(key, part):
    head_order = jax.random.permutation(jax.random.fold_in(key, 5), ASKER_HEAD_TOTAL)
    fast_heads = head_order < ASKER_HEAD_TOTAL // 2
    slow_rate = jnp.exp(jax.random.uniform(jax.random.fold_in(key, 6), (ASKER_HEAD_TOTAL,), jnp.float32, math.log(0.2), math.log(0.6))) / MIXER_SEQ_SPAN
    fast_rate = jnp.exp(jax.random.uniform(jax.random.fold_in(key, 7), (ASKER_HEAD_TOTAL,), jnp.float32, math.log(0.01), math.log(1.0 / 30.0)))
    step_rate = jnp.where(fast_heads, fast_rate, slow_rate)
    blocks = jnp.exp(jax.random.uniform(jax.random.fold_in(key, 8), (MIXER_SEQ_SPAN // ATT_ROWS,), jnp.float32, math.log(0.4), math.log(2.5)))
    per_block = jnp.repeat(blocks, ATT_ROWS)
    jitter = jax.random.uniform(jax.random.fold_in(key, 9), (ASKER_HEAD_TOTAL, MIXER_SEQ_SPAN), jnp.float32, 0.2, 1.8)
    decay_log_steps = step_rate[:, None] * per_block[None, :] * jitter
    decay_span_offset = jax.random.randint(jax.random.fold_in(key, 10), (ASKER_HEAD_TOTAL, 2), 0, MIXER_SEQ_SPAN)
    decay_span_size = jax.random.uniform(jax.random.fold_in(key, 12), (ASKER_HEAD_TOTAL, 2), jnp.float32, 0.22, 0.69)
    sequence_slot_number = jnp.arange(MIXER_SEQ_SPAN, dtype=jnp.int32)
    for decay_span_values in range(2):
        decay_log_steps = decay_log_steps + jnp.where(sequence_slot_number[None, :] == decay_span_offset[:, decay_span_values:decay_span_values + 1], decay_span_size[:, decay_span_values:decay_span_values + 1], 0.0)
    return -jnp.cumsum(decay_log_steps, axis=1)


def draw_expert_tokens(key, part):
    scale_top = math.log(10.0)
    result = base_values(jax.random.fold_in(key, 13), (TOK_EXP, D))
    row_scale = jnp.exp(jax.random.uniform(jax.random.fold_in(key, 14), (TOK_EXP, 1), jnp.float32, 0.0, math.log(10.0)))
    column_scale = jnp.exp(jax.random.uniform(jax.random.fold_in(key, 15), (1, D), jnp.float32, 0.0, scale_top))
    return (result * row_scale * column_scale).astype(jnp.bfloat16)


def draw_route_logits(key, part):
    result = base_values(jax.random.fold_in(key, 16), (TOK_EXP, TOPK))
    return result


def steps_of(stream_key, extent, shards, least, high):
    def one(dim, parts):
        heights = jax.random.uniform(jax.random.fold_in(jax.random.fold_in(stream_key, 6), dim), (parts,), jnp.float32, least / len(shards), high / len(shards))
        return jnp.repeat(jnp.exp(heights), extent[dim] // parts).reshape((-1,) + (1,) * (len(extent) - dim - 1))

    factor_of = one(*shards[0])
    for cut in shards[1:]:
        factor_of = factor_of * one(*cut)
    return factor_of


def deal_out(own_key, own, number, rows, count, top, limit, skew):
    sequence = jax.random.permutation(own_key, count)
    heavy_load, common = portions_of(count, rows * top, limit, skew, True), portions_of(count, rows * top, limit, skew, False)
    places = jnp.arange(count)

    def named(sizes, turn):
        used = int((sizes > 0).sum())
        fixed = max(1, used // 4)
        passed = fixed + (places - fixed + turn * (used - fixed)) % max(1, count - fixed)
        return jnp.zeros((count,), jnp.int32).at[sequence[jnp.where(places < fixed, places, passed)]].set(jnp.asarray(sizes, jnp.int32))

    sizes = jnp.where(number % 4 == 0, named(heavy_load, number // 4), named(common, number - number // 4 - 1))
    mixed = jax.random.permutation(jax.random.fold_in(own, 3), count)
    source_of, taker = mixed[0:count // 2 * 2:2], mixed[1:count // 2 * 2:2]
    slack = jnp.minimum(sizes[source_of] - 1, limit - sizes[taker]) // 2
    slack = jnp.where((source_of == sequence[0]) | (taker == sequence[0]) | (sizes[taker] == 0), 0, jnp.maximum(slack, 0))
    passed = jax.random.randint(jax.random.fold_in(own, 4), (count // 2,), 0, 1 << 20) % (slack + 1)
    sizes = sizes.at[source_of].add(-passed).at[taker].add(passed)
    items = jnp.searchsorted(jnp.cumsum(sizes), jnp.arange(rows * top), side="right").astype(jnp.int32)
    listing = items.reshape(top, rows).T
    listing = listing[jax.random.permutation(jax.random.fold_in(own, 1), rows)]
    turn = jax.random.randint(jax.random.fold_in(own, 2), (rows, 1), 0, top)
    return jnp.take_along_axis(listing, (jnp.arange(top)[None, :] + turn) % top, axis=1)


def portions_of(amount, total, bound, skew, full):
    portions = [(1 << 20) // math.isqrt(rank ** skew) + 1 for rank in range(1, amount + 1)]
    largest = bound if full else min(bound, max(-(-total // amount), total * portions[0] // sum(portions)))
    least = 1 if total - largest >= amount - 1 else 0
    given, surplus = [largest] + [least] * (amount - 1), total - largest - least * (amount - 1)
    while surplus > 0:
        movable = [i for i in range(1, amount) if given[i] < largest] or [i for i in range(1, amount) if given[i] < bound]
        whole, remaining = sum([portions[i] for i in movable]), surplus
        for i in movable:
            extra = min(bound - given[i], max(1, remaining * portions[i] // whole), surplus)
            given[i] = given[i] + extra
            surplus = surplus - extra
    return np.array(given)


def noise(own_key, dims, deviation, most, cuts=(), held_as=jnp.bfloat16):
    loudness = steps_of(own_key, dims, cuts, -0.22, 0.18) if cuts else 1.0
    values = jax.random.normal(own_key, dims, jnp.float32) * deviation * loudness
    return jnp.minimum(jnp.maximum(values, -most), most).astype(held_as)


def setup_inputs(seed: int = 0) -> dict:
    streams_of = jax.random.split(jax.random.key(seed), 13)
    queries = draw_queries(jax.random.fold_in(streams_of[12], 71), 0)
    keys_values = draw_keys_values(jax.random.fold_in(streams_of[12], 71), 0)
    forget_cache = draw_forget_cache(jax.random.fold_in(streams_of[12], 71), 0)
    heads_gain = jnp.clip(1.0 + 0.18 * jax.random.normal(streams_of[3], (ASKER_HEAD_TOTAL * HEAD,), jnp.float32), 0.1, 1.9)
    output_weight = noise(streams_of[4], (ASKER_HEAD_TOTAL * HEAD, D), (ASKER_HEAD_TOTAL * HEAD) ** -0.5, 0.1875)
    expert_tokens = draw_expert_tokens(jax.random.fold_in(streams_of[12], 71), 0)
    expert_gain = jnp.clip(1.0 + 0.18 * jax.random.normal(streams_of[6], (D,), jnp.float32), 0.1, 1.9)
    routes_keys = jax.random.split(jax.random.fold_in(streams_of[7], 1), TOK_EXP // EXP_ROWS)
    routes_turns = jax.random.permutation(jax.random.fold_in(streams_of[7], 3), TOK_EXP // EXP_ROWS)
    routes = jax.vmap(lambda own, number: deal_out(jax.random.fold_in(streams_of[7], 2), own, number, EXP_ROWS, EXPERTS, TOPK, CAP, 2))(routes_keys, routes_turns).reshape((TOK_EXP, TOPK))
    route_logits = draw_route_logits(jax.random.fold_in(streams_of[12], 71), 0)
    gate_weight = noise(streams_of[9], (EXPERTS, D, FF), (D // 16) ** -0.5, 0.5, ((0, 32), (2, 8)))
    up_weight = noise(streams_of[10], (EXPERTS, D, FF), (D // 16) ** -0.5, 0.5, ((0, 32), (2, 8)))
    down_weight = noise(streams_of[11], (EXPERTS, FF, D), (FF * 64) ** -0.5, 0.015625, ((0, 32), (1, 8)))
    return {"queries": queries, "keys_values": keys_values, "forget_cache": forget_cache, "heads_gain": heads_gain, "output_weight": output_weight, "expert_tokens": expert_tokens, "expert_gain": expert_gain, "routes": routes, "route_logits": route_logits, "gate_weight": gate_weight, "up_weight": up_weight, "down_weight": down_weight}


epsilon = 1e-06
clamp_limit = 7.0
sigmoid_slope = 1.702

def scaled_rows(values, gain_vector):
    as_float = values.astype(jnp.float32)
    inverse = lax.rsqrt(lax.optimization_barrier(jnp.mean(as_float * as_float, axis=-1, keepdims=True)) + epsilon)
    return (as_float * inverse * gain_vector.astype(jnp.float32)).astype(jnp.bfloat16)

def assign_slots(routes, experts, capacity):
    row_count, pick_count = routes.shape
    flat_routes = routes.reshape(-1)
    onehot = (flat_routes[:, None] == jnp.arange(experts, dtype=jnp.int32)[None, :]).astype(jnp.int32)
    earlier = jnp.cumsum(onehot, axis=0) - onehot
    slot_rank = lax.optimization_barrier(jnp.sum(earlier * onehot, axis=1)).astype(jnp.int32)
    position = (flat_routes * capacity + slot_rank).astype(jnp.int32)
    owner_row = (jnp.arange(row_count * pick_count, dtype=jnp.int32) // pick_count).astype(jnp.int32)
    slot_token = jnp.full((experts * capacity,), row_count, jnp.int32).at[position].set(owner_row)
    return (position.reshape(row_count, pick_count), slot_token)

def reference(queries, keys_values, forget_cache, heads_gain, output_weight, expert_tokens, expert_gain, routes, route_logits, gate_weight, up_weight, down_weight):
    group_size = ASKER_HEAD_TOTAL // KV_HEADS
    key_pairs = keys_values.reshape(MIXER_SEQ_SPAN, KV_HEADS, 2 * HEAD)
    query_heads = queries.reshape(MIXER_SEQ_SPAN, ASKER_HEAD_TOTAL, HEAD)
    block_width = math.gcd(MIXER_SEQ_SPAN, 512)
    key_pos = jnp.arange(MIXER_SEQ_SPAN, dtype=jnp.int32)
    score_scale = 1.0 / math.sqrt(HEAD)

    def one_head(head_number):
        key_head = head_number // group_size
        key_rows = key_pairs[:, key_head, :HEAD]
        value_rows = key_pairs[:, key_head, HEAD:]
        gate_row = forget_cache[head_number]
        query_all = query_heads[:, head_number, :]

        def one_block(block_index):
            first_row = block_index * block_width
            query_rows = lax.dynamic_slice_in_dim(query_all, first_row, block_width, 0)
            query_gate = lax.dynamic_slice_in_dim(gate_row, first_row, block_width, 0)
            scores = jnp.dot(query_rows, key_rows.T, preferred_element_type=jnp.float32) * score_scale
            scores = scores + query_gate[:, None] - gate_row[None, :]
            query_pos = first_row + jnp.arange(block_width, dtype=jnp.int32)
            scores = jnp.where(key_pos[None, :] <= query_pos[:, None], scores, -jnp.inf)
            row_max = lax.optimization_barrier(jnp.max(scores, axis=1, keepdims=True))
            weights = jnp.exp(scores - row_max)
            denominator = lax.optimization_barrier(jnp.sum(weights, axis=1, keepdims=True))
            summed = jnp.dot(weights.astype(jnp.bfloat16), value_rows, preferred_element_type=jnp.float32)
            return (summed / denominator).astype(jnp.bfloat16)
        return lax.map(one_block, jnp.arange(MIXER_SEQ_SPAN // block_width, dtype=jnp.int32)).reshape(MIXER_SEQ_SPAN, HEAD)
    attended = lax.map(one_head, jnp.arange(ASKER_HEAD_TOTAL, dtype=jnp.int32))
    attended = jnp.transpose(attended, (1, 0, 2)).reshape(MIXER_SEQ_SPAN, ASKER_HEAD_TOTAL * HEAD)
    heads_normed = scaled_rows(attended, heads_gain)
    mixer_out = jnp.dot(heads_normed, output_weight, preferred_element_type=jnp.float32).astype(jnp.bfloat16)
    expert_in = scaled_rows(expert_tokens, expert_gain)
    shifted = route_logits - lax.optimization_barrier(jnp.max(route_logits, axis=1, keepdims=True))
    raised = jnp.exp(shifted)
    route_weight = raised / lax.optimization_barrier(jnp.sum(raised, axis=1, keepdims=True))
    block_routes = routes.reshape(N_EP, EXP_ROWS, TOPK)
    block_weights = route_weight.reshape(N_EP, EXP_ROWS, TOPK)
    position, slot_token = jax.vmap(lambda chosen: assign_slots(chosen, EXPERTS, CAP))(block_routes)
    block_base = (jnp.arange(N_EP, dtype=jnp.int32) * EXP_ROWS)[:, None]
    global_token = jnp.where(slot_token < EXP_ROWS, slot_token + block_base, TOK_EXP).astype(jnp.int32)

    def weight_table(place, weights):
        return jnp.zeros((EXPERTS * CAP,), jnp.float32).at[place.reshape(-1)].set(weights.reshape(-1))
    slot_weight = jax.vmap(weight_table)(position, block_weights)
    padded = jnp.concatenate([expert_in, jnp.zeros((1, D), jnp.bfloat16)], axis=0)
    ff_block = FF // N_TP

    def accumulate(combined, expert):
        token_index = lax.dynamic_slice_in_dim(global_token, expert * CAP, CAP, 1).reshape(-1)
        slot_scale = lax.dynamic_slice_in_dim(slot_weight, expert * CAP, CAP, 1).reshape(-1)
        rows_in = jnp.take(padded, token_index, axis=0)
        gate_pre = jnp.dot(rows_in, gate_weight[expert], preferred_element_type=jnp.float32)
        up_pre = jnp.dot(rows_in, up_weight[expert], preferred_element_type=jnp.float32)
        gate_cut = jnp.minimum(gate_pre, clamp_limit)
        up_cut = jnp.clip(up_pre, -clamp_limit, clamp_limit)
        hidden = ((up_cut + 1.0) * gate_cut * jax.nn.sigmoid(sigmoid_slope * gate_cut)).astype(jnp.bfloat16)
        down_local = down_weight[expert]
        expert_sum = jnp.zeros((N_EP * CAP, D), jnp.float32)
        for block_index in range(N_TP):
            partial_value = jnp.dot(hidden[:, block_index * ff_block:(block_index + 1) * ff_block], down_local[block_index * ff_block:(block_index + 1) * ff_block, :], preferred_element_type=jnp.float32).astype(jnp.bfloat16)
            expert_sum = expert_sum + partial_value.astype(jnp.float32)
        expert_out = expert_sum.astype(jnp.bfloat16)
        combined = combined.at[token_index].add(expert_out.astype(jnp.float32) * slot_scale[:, None])
        return (combined, None)
    combined, _ = lax.scan(accumulate, jnp.zeros((TOK_EXP + 1, D), jnp.float32), jnp.arange(EXPERTS, dtype=jnp.int32))
    moe_out = combined[:TOK_EXP].astype(jnp.bfloat16)
    return (mixer_out, moe_out)
```

```python
import math

import jax
import jax.numpy as jnp
from jax import lax
from jax.sharding import Mesh
from jax.experimental import pallas as pl
from jax.experimental.pallas import tpu as pltpu
from jax.sharding import PartitionSpec as P

HEAD = 64
EP = ("ep_0", "ep_1")
EP_TP = ("ep_0", "ep_1", "tp")


epsilon = 1e-06
clamp_limit = 7.0
sigmoid_slope = 1.702


def gathered_by_axis(array, axes, dim):
    whole = array
    for number in range(len(axes) - 1, -1, -1):
        whole = lax.all_gather(whole, axes[number], axis=dim, tiled=True)
    return whole


def in_blocks(array, dim, devices):
    before, after = (array.shape[:dim], array.shape[dim + 1 :])
    return jnp.moveaxis(array.reshape(*before, devices, -1, *after), dim, 0)


def sent_and_summed(array, axis, dim):
    devices = lax.axis_size(axis)
    parts = lax.all_to_all(in_blocks(array, dim, devices), axis, 0, 0, tiled=True)
    return jnp.sum(parts.astype(jnp.float32), axis=0)


def scaled_rows(values, gain_vector):
    as_float = values.astype(jnp.float32)
    inverse = lax.rsqrt(jnp.mean(as_float * as_float, axis=-1, keepdims=True) + epsilon)
    return (as_float * inverse * gain_vector).astype(jnp.bfloat16)


def split3(x):
    hi = x.astype(jnp.bfloat16)
    rest = x - hi.astype(jnp.float32)
    mid = rest.astype(jnp.bfloat16)
    low = (rest - mid.astype(jnp.float32)).astype(jnp.bfloat16)
    return hi, mid, low


ROWS = 512
ASKED = 2 * ROWS
TILE = 256


def query_operand(query_rows, qx):
    turned = (query_rows.astype(jnp.float32) * (1.0 / math.sqrt(HEAD))).T.astype(jnp.bfloat16)
    row = lax.broadcasted_iota(jnp.int32, (HEAD, ASKED), 0)
    col = lax.broadcasted_iota(jnp.int32, (HEAD, ASKED), 1)
    first = (col < ROWS) & (row < 3)
    second = (col >= ROWS) & (row >= 3) & (row < 6)
    qx[0:HEAD, 0:ROWS] = turned[0:HEAD]
    qx[0:HEAD, ROWS:ASKED] = turned[HEAD : 2 * HEAD]
    qx[HEAD : 2 * HEAD, :] = jnp.where(first | second, -1.0, 0.0).astype(jnp.bfloat16)


def key_operand(block_rows, gate):
    hi, mid, low = split3(gate)
    parts = jnp.concatenate(
        [hi[0:1], mid[0:1], low[0:1], hi[1:2], mid[1:2], low[1:2]], axis=0
    ).astype(jnp.float32)
    full = jnp.concatenate(
        [jnp.zeros((64, ROWS), jnp.float32), parts, jnp.zeros((58, ROWS), jnp.float32)], axis=0
    )
    lane = lax.broadcasted_iota(jnp.int32, (ROWS, 2 * HEAD), 1)
    return jnp.where(lane < HEAD, block_rows, full.T.astype(jnp.bfloat16))


def value_operand(block_rows):
    turned = block_rows.astype(jnp.float32).T[HEAD : 2 * HEAD].astype(jnp.bfloat16)
    return jnp.concatenate([turned, jnp.ones((16, ROWS), jnp.bfloat16)], axis=0)


def attention_kernel(own_ref, q_ref, f_ref, kv_ref, o_ref, qx, top, acc, s_ref):
    own = own_ref[0]
    query_operand(q_ref[...], qx)
    base = pl.multiple_of(own * ROWS, ROWS)
    start = f_ref[:, pl.ds(base, 128)][:, 0:1]
    top[...] = jnp.full_like(top, -jnp.inf)
    acc[...] = jnp.zeros_like(acc)

    def rows_of(block):
        return pl.ds(pl.multiple_of(block * ROWS, ROWS), ROWS)

    keys = key_operand(kv_ref[rows_of(own), :], f_ref[:, rows_of(own)] - start)
    for tile in range(ASKED // TILE):
        cut = slice(tile * TILE, (tile + 1) * TILE)
        scores = jnp.dot(keys, qx[:, cut], preferred_element_type=jnp.float32)
        key_at = lax.broadcasted_iota(jnp.int32, (ROWS, TILE), 0)
        query_at = lax.broadcasted_iota(jnp.int32, (ROWS, TILE), 1) + (tile * TILE) % ROWS
        s_ref[0, :, cut] = jnp.where(key_at <= query_at, scores, -jnp.inf)

    def take(block, after, slot):
        keys = key_operand(kv_ref[rows_of(after), :], f_ref[:, rows_of(after)] - start)
        values = value_operand(kv_ref[rows_of(block), :])
        for tile in range(ASKED // TILE):
            cut = slice(tile * TILE, (tile + 1) * TILE)
            s_ref[1 - slot, :, cut] = jnp.dot(
                keys, qx[:, cut], preferred_element_type=jnp.float32
            )
            scores = s_ref[slot, :, cut]
            old = top[:, cut]
            new = jnp.maximum(old, jnp.max(scores, axis=0, keepdims=True))
            weights = jnp.exp(scores - new).astype(jnp.bfloat16)
            acc[:, cut] = acc[:, cut] * jnp.exp(old - new) + jnp.dot(
                values, weights, preferred_element_type=jnp.float32
            )
            top[:, cut] = new

    def pair(step, _):
        first = 2 * step
        take(jnp.where(first == 0, own, first - 1), jnp.minimum(first, jnp.maximum(own - 1, 0)), 0)

        @pl.when(first + 1 <= own)
        def _():
            take(first, jnp.minimum(first + 1, own - 1), 1)

        return 0

    lax.fori_loop(0, (own + 2) // 2, pair, 0)
    total = acc[...]
    result = total[0:HEAD] / total[HEAD : HEAD + 1]
    both = jnp.concatenate([result[:, 0:ROWS], result[:, ROWS:ASKED]], axis=0)
    o_ref[...] = both.T.astype(jnp.bfloat16)


def attention(own, queries, forget, whole):
    vmem = pl.BlockSpec(memory_space=pltpu.VMEM)
    return pl.pallas_call(
        attention_kernel,
        out_shape=jax.ShapeDtypeStruct((ROWS, 2 * HEAD), jnp.bfloat16),
        in_specs=[pl.BlockSpec(memory_space=pltpu.SMEM), vmem, vmem, vmem],
        out_specs=vmem,
        scratch_shapes=[
            pltpu.VMEM((2 * HEAD, ASKED), jnp.bfloat16),
            pltpu.VMEM((1, ASKED), jnp.float32),
            pltpu.VMEM((HEAD + 16, ASKED), jnp.float32),
            pltpu.VMEM((2, ROWS, ASKED), jnp.float32),
        ],
        compiler_params=pltpu.CompilerParams(vmem_limit_bytes=40 * 2**20),
        cost_estimate=pl.CostEstimate(
            flops=10**10, bytes_accessed=5 * 2**20, transcendentals=10**7
        ),
    )(own, queries, forget, whole)


def assign_slots(routes, experts, capacity):
    row_count, pick_count = routes.shape
    flat_routes = routes.reshape(-1)
    onehot = (flat_routes[:, None] == jnp.arange(experts, dtype=jnp.int32)[None, :]).astype(
        jnp.int32
    )
    earlier = jnp.cumsum(onehot, axis=0) - onehot
    slot_rank = jnp.sum(earlier * onehot, axis=1)
    position = flat_routes * capacity + slot_rank
    owner_row = jnp.arange(row_count * pick_count, dtype=jnp.int32) // pick_count
    slot_token = jnp.full((experts * capacity,), row_count, jnp.int32).at[position].set(owner_row)
    return (position.reshape(row_count, pick_count), slot_token)


def body(
    queries,
    keys_values,
    forget_cache,
    heads_gain,
    output_weight,
    expert_tokens,
    expert_gain,
    routes,
    route_logits,
    gate_weight,
    up_weight,
    down_weight,
):
    whole = gathered_by_axis(keys_values, EP, 0)
    own = lax.axis_index(EP).astype(jnp.int32).reshape(1)
    attended = attention(own, queries, forget_cache, whole)
    local_rows = lax.all_to_all(attended, "tp", split_axis=0, concat_axis=1, tiled=True)
    heads_normed = scaled_rows(local_rows, heads_gain)
    mixer_out = jnp.dot(heads_normed, output_weight, preferred_element_type=jnp.float32).astype(
        jnp.bfloat16
    )
    experts_count = lax.axis_size(EP)
    expert_rows, pick_count = routes.shape
    capacity = 2 * expert_rows * pick_count // experts_count
    expert_in = scaled_rows(expert_tokens, expert_gain)
    shifted = route_logits - jnp.max(route_logits, axis=1, keepdims=True)
    raised = jnp.exp(shifted)
    route_weight = raised / jnp.sum(raised, axis=1, keepdims=True)
    position, slot_token = assign_slots(routes, experts_count, capacity)
    model_width = expert_in.shape[1]
    part_width = model_width // lax.axis_size("tp")
    gate_local = gate_weight[0]
    up_local = up_weight[0]
    down_local = down_weight[0]
    own_columns = lax.dynamic_slice_in_dim(
        expert_in, lax.axis_index("tp") * part_width, part_width, 1
    )
    padded = jnp.concatenate([own_columns, jnp.zeros((1, part_width), jnp.bfloat16)], axis=0)
    outgoing = jnp.take(padded, slot_token, axis=0).reshape(experts_count, capacity, part_width)
    arrived = lax.all_to_all(outgoing, EP, split_axis=0, concat_axis=0, tiled=True).reshape(
        experts_count * capacity, part_width
    )
    piece_rows = lax.all_gather(arrived, "tp", axis=1, tiled=True)
    gate_sum = jnp.dot(piece_rows, gate_local, preferred_element_type=jnp.float32)
    up_sum = jnp.dot(piece_rows, up_local, preferred_element_type=jnp.float32)
    gate_cut = jnp.minimum(gate_sum, clamp_limit)
    up_cut = jnp.clip(up_sum, -clamp_limit, clamp_limit)
    hidden = ((up_cut + 1.0) * gate_cut * jax.nn.sigmoid(sigmoid_slope * gate_cut)).astype(
        jnp.bfloat16
    )
    expert_out = sent_and_summed(
        lax.dot_general(
            down_local, hidden, (((0,), (1,)), ((), ())), preferred_element_type=jnp.float32
        ).astype(jnp.bfloat16),
        "tp",
        0,
    ).astype(jnp.bfloat16)
    returned = lax.all_to_all(expert_out, EP, split_axis=1, concat_axis=1, tiled=True)
    picked = jnp.take(returned, position.reshape(-1), axis=1).reshape(
        part_width, expert_rows, pick_count
    )
    moe_out = jnp.einsum("crk,rk->rc", picked.astype(jnp.float32), route_weight).astype(
        jnp.bfloat16
    )
    return (mixer_out, moe_out)


def solution(mesh):
    torus = Mesh(mesh.devices.reshape(8, 4, mesh.shape["tp"]), ("ep_0", "ep_1", "tp"))
    return jax.shard_map(
        body,
        mesh=torus,
        in_specs=(
            P(EP, "tp"),
            P(EP, "tp"),
            P("tp", None),
            P(),
            P(),
            P(EP, None),
            P(),
            P(EP, None),
            P(EP, None),
            P(EP, None, "tp"),
            P(EP, None, "tp"),
            P(EP, "tp", None),
        ),
        out_specs=(P(EP_TP, None), P(EP, "tp")),
        check_vma=False,
    )
```

```python
import math

import jax
import jax.numpy as jnp
from jax import lax
from jax.sharding import Mesh
from jax.experimental import pallas as pl
from jax.experimental.pallas import tpu as pltpu
from jax.sharding import PartitionSpec as P

HEAD = 64
EP = ("ep_0", "ep_1")
EP_TP = ("ep_0", "ep_1", "tp")


epsilon = 1e-06
clamp_limit = 7.0
sigmoid_slope = 1.702


def gathered_by_axis(array, axes, dim):
    whole = array
    for number in range(len(axes) - 1, -1, -1):
        whole = lax.all_gather(whole, axes[number], axis=dim, tiled=True)
    return whole


def scaled_rows(values, gain_vector):
    as_float = values.astype(jnp.float32)
    inverse = lax.rsqrt(jnp.mean(as_float * as_float, axis=-1, keepdims=True) + epsilon)
    return (as_float * inverse * gain_vector).astype(jnp.bfloat16)


def split3(x):
    hi = x.astype(jnp.bfloat16)
    rest = x - hi.astype(jnp.float32)
    mid = rest.astype(jnp.bfloat16)
    low = (rest - mid.astype(jnp.float32)).astype(jnp.bfloat16)
    return hi, mid, low


ROWS = 512
ASKED = 2 * ROWS
TILE = 256


def query_operand(query_rows, qx):
    turned = (query_rows.astype(jnp.float32) * (1.0 / math.sqrt(HEAD))).T.astype(jnp.bfloat16)
    row = lax.broadcasted_iota(jnp.int32, (HEAD, ASKED), 0)
    col = lax.broadcasted_iota(jnp.int32, (HEAD, ASKED), 1)
    first = (col < ROWS) & (row < 3)
    second = (col >= ROWS) & (row >= 3) & (row < 6)
    qx[0:HEAD, 0:ROWS] = turned[0:HEAD]
    qx[0:HEAD, ROWS:ASKED] = turned[HEAD : 2 * HEAD]
    qx[HEAD : 2 * HEAD, :] = jnp.where(first | second, -1.0, 0.0).astype(jnp.bfloat16)


def key_operand(block_rows, gate):
    hi, mid, low = split3(gate)
    parts = jnp.concatenate(
        [hi[0:1], mid[0:1], low[0:1], hi[1:2], mid[1:2], low[1:2]], axis=0
    ).astype(jnp.float32)
    full = jnp.concatenate(
        [jnp.zeros((64, ROWS), jnp.float32), parts, jnp.zeros((58, ROWS), jnp.float32)], axis=0
    )
    lane = lax.broadcasted_iota(jnp.int32, (ROWS, 2 * HEAD), 1)
    return jnp.where(lane < HEAD, block_rows, full.T.astype(jnp.bfloat16))


def value_operand(block_rows):
    turned = block_rows.astype(jnp.float32).T[HEAD : 2 * HEAD].astype(jnp.bfloat16)
    return jnp.concatenate([turned, jnp.ones((16, ROWS), jnp.bfloat16)], axis=0)


def attention_kernel(own_ref, q_ref, f_ref, kv_ref, later_ref, o_ref, qx, top, acc, s_ref):
    own = own_ref[0]
    query_operand(q_ref[...], qx)
    base = pl.multiple_of(own * ROWS, ROWS)
    start = f_ref[:, pl.ds(base, 128)][:, 0:1]
    top[...] = jnp.full_like(top, -jnp.inf)
    acc[...] = jnp.zeros_like(acc)

    def rows_of(block):
        return pl.ds(pl.multiple_of(block * ROWS, ROWS), ROWS)

    keys = key_operand(kv_ref[rows_of(own), :], f_ref[:, rows_of(own)] - start)
    for tile in range(ASKED // TILE):
        cut = slice(tile * TILE, (tile + 1) * TILE)
        scores = jnp.dot(keys, qx[:, cut], preferred_element_type=jnp.float32)
        key_at = lax.broadcasted_iota(jnp.int32, (ROWS, TILE), 0)
        query_at = lax.broadcasted_iota(jnp.int32, (ROWS, TILE), 1) + (tile * TILE) % ROWS
        s_ref[0, :, cut] = jnp.where(key_at <= query_at, scores, -jnp.inf)

    def take(block, after, slot):
        keys = key_operand(kv_ref[rows_of(after), :], f_ref[:, rows_of(after)] - start)
        values = value_operand(kv_ref[rows_of(block), :])
        for tile in range(ASKED // TILE):
            cut = slice(tile * TILE, (tile + 1) * TILE)
            s_ref[1 - slot, :, cut] = jnp.dot(
                keys, qx[:, cut], preferred_element_type=jnp.float32
            )
            scores = s_ref[slot, :, cut]
            old = top[:, cut]
            new = jnp.maximum(old, jnp.max(scores, axis=0, keepdims=True))
            weights = jnp.exp(scores - new).astype(jnp.bfloat16)
            acc[:, cut] = acc[:, cut] * jnp.exp(old - new) + jnp.dot(
                values, weights, preferred_element_type=jnp.float32
            )
            top[:, cut] = new

    def pair(step, _):
        first = 2 * step
        take(jnp.where(first == 0, own, first - 1), jnp.minimum(first, jnp.maximum(own - 1, 0)), 0)

        @pl.when(first + 1 <= own)
        def _():
            take(first, jnp.minimum(first + 1, own - 1), 1)

        return 0

    lax.fori_loop(0, (own + 2) // 2, pair, 0)
    total = acc[...]
    result = total[0:HEAD] / total[HEAD : HEAD + 1]
    both = jnp.concatenate([result[:, 0:ROWS], result[:, ROWS:ASKED]], axis=0)
    o_ref[...] = both.T.astype(jnp.bfloat16)


def attention(own, queries, forget, whole, later):
    vmem = pl.BlockSpec(memory_space=pltpu.VMEM)
    return pl.pallas_call(
        attention_kernel,
        out_shape=jax.ShapeDtypeStruct((ROWS, 2 * HEAD), jnp.bfloat16),
        in_specs=[
            pl.BlockSpec(memory_space=pltpu.SMEM),
            vmem,
            vmem,
            vmem,
            pl.BlockSpec(memory_space=pl.ANY),
        ],
        out_specs=vmem,
        scratch_shapes=[
            pltpu.VMEM((2 * HEAD, ASKED), jnp.bfloat16),
            pltpu.VMEM((1, ASKED), jnp.float32),
            pltpu.VMEM((HEAD + 16, ASKED), jnp.float32),
            pltpu.VMEM((2, ROWS, ASKED), jnp.float32),
        ],
        compiler_params=pltpu.CompilerParams(vmem_limit_bytes=40 * 2**20),
        cost_estimate=pl.CostEstimate(
            flops=10**10, bytes_accessed=5 * 2**20, transcendentals=10**7
        ),
    )(own, queries, forget, whole, later)


MESH = pl.DeviceIdType.MESH
EXPERTS = 32
SLOTS = 32
TOKENS = 128
WIDTH = 2048
PART = 256
ALL_SLOTS = EXPERTS * SLOTS
CHUNKS = 4
CHUNK = ALL_SLOTS // CHUNKS
PER_CHUNK = CHUNK // SLOTS
HALF = CHUNK // 2


def offset_at(position):
    return (position + 1) // 2 if position % 2 else (EXPERTS - position // 2) % EXPERTS


def mirror(position):
    if position in (0, EXPERTS - 1):
        return position
    return position + 1 if position % 2 else position - 1


def landed(ref, sem):
    pltpu.make_async_copy(ref, ref, sem).wait()


def moe_kernel(
    tokens,
    gain,
    routes,
    logits,
    gate_hbm,
    up_hbm,
    down_hbm,
    out,
    gate,
    up,
    down,
    place,
    weigh,
    outgoing,
    features,
    partial,
    paired,
    passed,
    reached,
    result,
    returned,
    load_sem,
    go_send,
    go_recv,
    ag_send,
    ag_recv,
    rs_send,
    rs_recv,
    back_send,
    back_recv,
):
    z, x, t = lax.axis_index("ep_0"), lax.axis_index("ep_1"), lax.axis_index("tp")
    me = z * 4 + x
    y, core = t // 2, t % 2
    above = ((y + 1) % 4) * 2 + core
    below = ((y + 3) % 4) * 2 + core
    across = ((y + 2) % 4) * 2 + core
    beside = y * 2 + (1 - core)

    def twin(number):
        return (number // 2) * 2 + 1 - core

    def along(offset):
        peer = (me + offset) % EXPERTS
        return {"ep_0": peer // 4, "ep_1": peer % 4}

    barrier = pltpu.get_barrier_semaphore()
    for offset in range(1, EXPERTS):
        pl.semaphore_signal(barrier, inc=1, device_id=along(offset), device_id_type=MESH)
    for offset in range(1, 8):
        pl.semaphore_signal(
            barrier, inc=1, device_id={"tp": (t + offset) % 8}, device_id_type=MESH
        )
    loads = [
        pltpu.make_async_copy(source, target, load_sem.at[number])
        for number, (source, target) in enumerate(((gate_hbm, gate), (up_hbm, up), (down_hbm, down)))
    ]
    for load in loads:
        load.start()

    values = tokens[...].astype(jnp.float32)
    inverse = lax.rsqrt(jnp.mean(values * values, axis=1, keepdims=True) + epsilon)
    columns = pl.ds(pl.multiple_of(t * PART, PART), PART)
    own = (tokens[:, columns].astype(jnp.float32) * inverse * gain[:, columns]).astype(
        jnp.bfloat16
    )
    picks = routes[...]
    raised = jnp.exp(logits[...] - jnp.max(logits[...], axis=0, keepdims=True))
    route_weight = raised / jnp.sum(raised, axis=0, keepdims=True)
    number = lax.broadcasted_iota(jnp.int32, (EXPERTS, TOKENS), 0)
    offset = jnp.where(number % 2 == 1, (number + 1) // 2, (EXPERTS - number // 2) % EXPERTS)
    expert = (me + offset) % EXPERTS
    named = jnp.zeros((EXPERTS, TOKENS), jnp.float32)
    share = jnp.zeros((EXPERTS, TOKENS), jnp.float32)
    for pick in range(4):
        same = picks[pick : pick + 1, :] == expert
        named = named + jnp.where(same, 1.0, 0.0)
        share = share + jnp.where(same, route_weight[pick : pick + 1, :], 0.0)
    before = (
        lax.broadcasted_iota(jnp.int32, (TOKENS, TOKENS), 0)
        < lax.broadcasted_iota(jnp.int32, (TOKENS, TOKENS), 1)
    )
    rank = jnp.dot(
        named.astype(jnp.bfloat16),
        jnp.where(before, 1.0, 0.0).astype(jnp.bfloat16),
        preferred_element_type=jnp.float32,
    )
    slot = jnp.where(named > 0.0, rank, -1.0)
    share_high = share.astype(jnp.bfloat16).astype(jnp.float32)
    share_low = share - share_high
    level = lax.broadcasted_iota(jnp.int32, (SLOTS, TOKENS), 0).astype(jnp.float32)
    for position in range(EXPERTS):
        hit = level == slot[position : position + 1, :]
        rows = slice(position * SLOTS, (position + 1) * SLOTS)
        place[rows, :] = jnp.where(hit, 1.0, 0.0).astype(jnp.bfloat16)
        weigh[0, rows, :] = jnp.where(hit, share_high[position : position + 1, :], 0.0).astype(
            jnp.bfloat16
        )
        weigh[1, rows, :] = jnp.where(hit, share_low[position : position + 1, :], 0.0).astype(
            jnp.bfloat16
        )
    outgoing[...] = jnp.dot(place[...], own, preferred_element_type=jnp.float32).astype(
        jnp.bfloat16
    )
    features[t, 0:SLOTS, :] = outgoing[0:SLOTS, :]
    pl.semaphore_wait(barrier, EXPERTS - 1 + 7)

    started = []

    def send(source, target, send_sem, recv_sem, device):
        copy = pltpu.make_async_remote_copy(
            src_ref=source,
            dst_ref=target,
            send_sem=send_sem,
            recv_sem=recv_sem,
            device_id=device,
            device_id_type=MESH,
        )
        copy.start()
        started.append(copy)

    def slots(position):
        return pl.ds(position * SLOTS, SLOTS)

    for position in range(1, EXPERTS):
        landing = mirror(position)
        send(
            outgoing.at[slots(position)],
            features.at[t, slots(landing)],
            go_send.at[position],
            go_recv.at[landing],
            along(offset_at(position)),
        )

    def rows_of(chunk):
        return pl.ds(chunk * CHUNK, CHUNK)

    def spread(chunk):
        for position in range(chunk * PER_CHUNK, (chunk + 1) * PER_CHUNK):
            if position:
                landed(features.at[t, slots(position)], go_recv.at[position])
        block = features.at[t, rows_of(chunk)]
        for kind, target in ((0, above), (1, below), (4, beside)):
            send(block, block, ag_send.at[chunk, kind], ag_recv.at[chunk, kind], {"tp": target})

    def forward(chunk):
        for kind, source, target, first in ((0, below, above, 0), (1, above, below, HALF)):
            block = features.at[source, rows_of(chunk)]
            landed(block, ag_recv.at[chunk, kind])
            part = features.at[source, pl.ds(chunk * CHUNK + first, HALF)]
            send(part, part, ag_send.at[chunk, 2 + kind], ag_recv.at[chunk, 2 + kind], {"tp": target})
            send(block, block, ag_send.at[chunk, 5 + kind], ag_recv.at[chunk, 5 + kind], {"tp": beside})

    def complete(chunk):
        for kind, first in ((2, 0), (3, HALF)):
            landed(
                features.at[across, pl.ds(chunk * CHUNK + first, HALF)], ag_recv.at[chunk, kind]
            )
        block = features.at[across, rows_of(chunk)]
        send(block, block, ag_send.at[chunk, 7], ag_recv.at[chunk, 7], {"tp": beside})

    def multiply(chunk):
        for kind, source in ((4, beside), (5, twin(below)), (6, twin(above)), (7, twin(across))):
            landed(features.at[source, rows_of(chunk)], ag_recv.at[chunk, kind])
        if chunk == 0:
            for load in loads:
                load.wait()
        gate_sum = jnp.zeros((CHUNK, PART), jnp.float32)
        up_sum = jnp.zeros((CHUNK, PART), jnp.float32)
        for source in range(8):
            rows = features[source, rows_of(chunk), :]
            depth = slice(source * PART, (source + 1) * PART)
            gate_sum = gate_sum + jnp.dot(rows, gate[depth, :], preferred_element_type=jnp.float32)
            up_sum = up_sum + jnp.dot(rows, up[depth, :], preferred_element_type=jnp.float32)
        gate_cut = jnp.minimum(gate_sum, clamp_limit)
        up_cut = jnp.clip(up_sum, -clamp_limit, clamp_limit)
        hidden = ((up_cut + 1.0) * gate_cut * jax.nn.sigmoid(sigmoid_slope * gate_cut)).astype(
            jnp.bfloat16
        )
        for other in (1, 0):
            for turn in range(4):
                target = ((y + turn) % 4) * 2 + ((1 - core) if other else core)
                partial[chunk, other, turn] = jnp.dot(
                    hidden,
                    down[:, pl.ds(pl.multiple_of(target * PART, PART), PART)],
                    preferred_element_type=jnp.float32,
                ).astype(jnp.bfloat16)
            if other:
                send(
                    partial.at[chunk, 1],
                    paired.at[chunk],
                    rs_send.at[chunk, 0],
                    rs_recv.at[chunk, 0],
                    {"tp": beside},
                )

    def added(*values):
        total = values[0].astype(jnp.float32)
        for value in values[1:]:
            total = total + value.astype(jnp.float32)
        return total.astype(jnp.bfloat16)

    def join(chunk):
        landed(paired.at[chunk], rs_recv.at[chunk, 0])
        partial[chunk, 0, 2] = added(partial[chunk, 0, 2], paired[chunk, 2])
        for kind, first, target in ((1, 0, above), (2, HALF, below)):
            send(
                partial.at[chunk, 0, 2, pl.ds(first, HALF)],
                passed.at[chunk, kind - 1],
                rs_send.at[chunk, kind],
                rs_recv.at[chunk, kind],
                {"tp": target},
            )
        for turn in (1, 3, 0):
            partial[chunk, 0, turn] = added(partial[chunk, 0, turn], paired[chunk, turn])

    def pass_on(chunk):
        for kind, turn, first, target in ((1, 1, 0, above), (2, 3, HALF, below)):
            landed(passed.at[chunk, kind - 1], rs_recv.at[chunk, kind])
            rows = slice(first, first + HALF)
            partial[chunk, 0, turn, rows] = added(
                partial[chunk, 0, turn, rows], passed[chunk, kind - 1]
            )
            send(
                partial.at[chunk, 0, turn],
                reached.at[chunk, kind - 1],
                rs_send.at[chunk, 2 + kind],
                rs_recv.at[chunk, 2 + kind],
                {"tp": target},
            )

    def finish(chunk):
        for kind in (3, 4):
            landed(reached.at[chunk, kind - 3], rs_recv.at[chunk, kind])
        result[rows_of(chunk), :] = added(
            partial[chunk, 0, 0], reached[chunk, 0], reached[chunk, 1]
        )
        for position in range(chunk * PER_CHUNK, (chunk + 1) * PER_CHUNK):
            if position == 0:
                returned[0:SLOTS, :] = result[0:SLOTS, :]
                continue
            landing = mirror(position)
            send(
                result.at[slots(position)],
                returned.at[slots(landing)],
                back_send.at[position],
                back_recv.at[landing],
                along(offset_at(position)),
            )

    plan = (
        (spread, 0), (spread, 1), (forward, 0), (spread, 2), (forward, 1), (complete, 0),
        (multiply, 0), (spread, 3), (forward, 2), (complete, 1), (join, 0), (multiply, 1),
        (forward, 3), (complete, 2), (pass_on, 0), (join, 1), (multiply, 2), (complete, 3),
        (finish, 0), (pass_on, 1), (join, 2), (multiply, 3), (finish, 1), (pass_on, 2),
        (join, 3), (finish, 2), (pass_on, 3), (finish, 3),
    )
    for step, chunk in plan:
        step(chunk)
    for position in range(1, EXPERTS):
        landed(returned.at[slots(position)], back_recv.at[position])
    turned = (((0,), (0,)), ((), ()))
    out[...] = (
        lax.dot_general(weigh[0], returned[...], turned, preferred_element_type=jnp.float32)
        + lax.dot_general(weigh[1], returned[...], turned, preferred_element_type=jnp.float32)
    ).astype(jnp.bfloat16)
    for copy in started:
        copy.wait_send()


def experts(tokens, gain, routes, logits, gate, up, down):
    vmem = pl.BlockSpec(memory_space=pltpu.VMEM)
    anywhere = pl.BlockSpec(memory_space=pl.ANY)
    half = jnp.bfloat16
    dma = pltpu.SemaphoreType.DMA
    return pl.pallas_call(
        moe_kernel,
        out_shape=jax.ShapeDtypeStruct((TOKENS, PART), half),
        in_specs=[vmem] * 4 + [anywhere] * 3,
        out_specs=vmem,
        scratch_shapes=[
            pltpu.VMEM((WIDTH, PART), half),
            pltpu.VMEM((WIDTH, PART), half),
            pltpu.VMEM((PART, WIDTH), half),
            pltpu.VMEM((ALL_SLOTS, TOKENS), half),
            pltpu.VMEM((2, ALL_SLOTS, TOKENS), half),
            pltpu.VMEM((ALL_SLOTS, PART), half),
            pltpu.VMEM((8, ALL_SLOTS, PART), half),
            pltpu.VMEM((CHUNKS, 2, 4, CHUNK, PART), half),
            pltpu.VMEM((CHUNKS, 4, CHUNK, PART), half),
            pltpu.VMEM((CHUNKS, 2, HALF, PART), half),
            pltpu.VMEM((CHUNKS, 2, CHUNK, PART), half),
            pltpu.VMEM((ALL_SLOTS, PART), half),
            pltpu.VMEM((ALL_SLOTS, PART), half),
            dma((3,)),
            dma((EXPERTS,)),
            dma((EXPERTS,)),
            dma((CHUNKS, 8)),
            dma((CHUNKS, 8)),
            dma((CHUNKS, 5)),
            dma((CHUNKS, 5)),
            dma((EXPERTS,)),
            dma((EXPERTS,)),
        ],
        compiler_params=pltpu.CompilerParams(
            collective_id=0, has_side_effects=True, vmem_limit_bytes=48 * 2**20
        ),
        cost_estimate=pl.CostEstimate(
            flops=4 * 10**10, bytes_accessed=2**23, transcendentals=10**6
        ),
    )(tokens, gain, routes, logits, gate, up, down)


def body(
    queries,
    keys_values,
    forget_cache,
    heads_gain,
    output_weight,
    expert_tokens,
    expert_gain,
    routes,
    route_logits,
    gate_weight,
    up_weight,
    down_weight,
):
    whole = gathered_by_axis(keys_values, EP, 0)
    moe_out = experts(
        expert_tokens,
        expert_gain.reshape(1, -1),
        routes.T,
        route_logits.T,
        gate_weight[0],
        up_weight[0],
        down_weight[0],
    )
    own = lax.axis_index(EP).astype(jnp.int32).reshape(1)
    attended = attention(own, queries, forget_cache, whole, moe_out)
    local_rows = lax.all_to_all(attended, "tp", split_axis=0, concat_axis=1, tiled=True)
    heads_normed = scaled_rows(local_rows, heads_gain)
    mixer_out = jnp.dot(heads_normed, output_weight, preferred_element_type=jnp.float32).astype(
        jnp.bfloat16
    )
    return (mixer_out, moe_out)


def solution(mesh):
    torus = Mesh(mesh.devices.reshape(8, 4, mesh.shape["tp"]), ("ep_0", "ep_1", "tp"))
    return jax.shard_map(
        body,
        mesh=torus,
        in_specs=(
            P(EP, "tp"),
            P(EP, "tp"),
            P("tp", None),
            P(),
            P(),
            P(EP, None),
            P(),
            P(EP, None),
            P(EP, None),
            P(EP, None, "tp"),
            P(EP, None, "tp"),
            P(EP, "tp", None),
        ),
        out_specs=(P(EP_TP, None), P(EP, "tp")),
        check_vma=False,
    )
```

```python
import math

import jax
import jax.numpy as jnp
from jax import lax
from jax.experimental import pallas as pl
from jax.experimental.pallas import tpu as pltpu
from jax.sharding import Mesh
from jax.sharding import PartitionSpec as P

HEAD = 64
EP = ("ep_0", "ep_1")
EP_TP = ("ep_0", "ep_1", "tp")


epsilon = 1e-06
clamp_limit = 7.0
sigmoid_slope = 1.702


def split3(x):
    hi = x.astype(jnp.bfloat16)
    rest = x - hi.astype(jnp.float32)
    mid = rest.astype(jnp.bfloat16)
    low = (rest - mid.astype(jnp.float32)).astype(jnp.bfloat16)
    return hi, mid, low


ROWS = 512
ASKED = 2 * ROWS
TILE = 256


def query_operand(query_rows, qx):
    turned = (query_rows.astype(jnp.float32) * (1.0 / math.sqrt(HEAD))).T.astype(jnp.bfloat16)
    row = lax.broadcasted_iota(jnp.int32, (HEAD, ASKED), 0)
    col = lax.broadcasted_iota(jnp.int32, (HEAD, ASKED), 1)
    first = (col < ROWS) & (row < 3)
    second = (col >= ROWS) & (row >= 3) & (row < 6)
    qx[0:HEAD, 0:ROWS] = turned[0:HEAD]
    qx[0:HEAD, ROWS:ASKED] = turned[HEAD : 2 * HEAD]
    qx[HEAD : 2 * HEAD, :] = jnp.where(first | second, -1.0, 0.0).astype(jnp.bfloat16)


def key_operand(block_rows, gate):
    hi, mid, low = split3(gate)
    parts = jnp.concatenate(
        [hi[0:1], mid[0:1], low[0:1], hi[1:2], mid[1:2], low[1:2]], axis=0
    ).astype(jnp.float32)
    full = jnp.concatenate(
        [jnp.zeros((64, ROWS), jnp.float32), parts, jnp.zeros((58, ROWS), jnp.float32)], axis=0
    )
    lane = lax.broadcasted_iota(jnp.int32, (ROWS, 2 * HEAD), 1)
    return jnp.where(lane < HEAD, block_rows, full.T.astype(jnp.bfloat16))


def value_operand(block_rows):
    turned = block_rows.astype(jnp.float32).T[HEAD : 2 * HEAD].astype(jnp.bfloat16)
    return jnp.concatenate([turned, jnp.ones((16, ROWS), jnp.bfloat16)], axis=0)


MESH = pl.DeviceIdType.MESH
EXPERTS = 32
SLOTS = 32
TOKENS = 128
WIDTH = 2048
PART = 256
ALL_SLOTS = EXPERTS * SLOTS
CHUNKS = 4
CHUNK = ALL_SLOTS // CHUNKS
PER_CHUNK = CHUNK // SLOTS
HALF = CHUNK // 2
PLANES = 8
FIRST = 320
SECOND = ROWS - FIRST
SHARE = ROWS // 8


def offset_at(position):
    return (position + 1) // 2 if position % 2 else (EXPERTS - position // 2) % EXPERTS


def mirror(position):
    if position in (0, EXPERTS - 1):
        return position
    return position + 1 if position % 2 else position - 1


def landed(ref, sem):
    pltpu.make_async_copy(ref, ref, sem).wait()


def kernel(
    tokens,
    gain,
    routes,
    logits,
    gate_hbm,
    up_hbm,
    down_hbm,
    queries,
    forget,
    heads_gain,
    own_hbm,
    mix_hbm,
    out,
    mixer_out,
    gate,
    up,
    down,
    place,
    weigh,
    outgoing,
    features,
    partial,
    paired,
    passed,
    reached,
    result,
    returned,
    mix,
    keys,
    qx,
    top,
    acc,
    s_ref,
    attended,
    gathered,
    load_sem,
    go_send,
    go_recv,
    ag_send,
    ag_recv,
    rs_send,
    rs_recv,
    back_send,
    back_recv,
    az_send,
    az_recv,
    ax_send,
    ax_recv,
    bx_send,
    bx_recv,
    bz_send,
    bz_recv,
    at_send,
    at_recv,
):
    z, x, t = lax.axis_index("ep_0"), lax.axis_index("ep_1"), lax.axis_index("tp")
    me = z * 4 + x
    y, core = t // 2, t % 2
    above = ((y + 1) % 4) * 2 + core
    below = ((y + 3) % 4) * 2 + core
    across = ((y + 2) % 4) * 2 + core
    beside = y * 2 + (1 - core)

    def twin(number):
        return (number // 2) * 2 + 1 - core

    def along(offset):
        peer = (me + offset) % EXPERTS
        return {"ep_0": peer // 4, "ep_1": peer % 4}

    barrier = pltpu.get_barrier_semaphore()
    for offset in range(1, EXPERTS):
        pl.semaphore_signal(barrier, inc=1, device_id=along(offset), device_id_type=MESH)
    for offset in range(1, 8):
        pl.semaphore_signal(
            barrier, inc=1, device_id={"tp": (t + offset) % 8}, device_id_type=MESH
        )
    loads = [
        pltpu.make_async_copy(source, target, load_sem.at[number])
        for number, (source, target) in enumerate(
            (
                (own_hbm, keys.at[me]),
                (gate_hbm, gate),
                (up_hbm, up),
                (down_hbm, down),
                (mix_hbm, mix),
            )
        )
    ]
    for load in loads:
        load.start()

    values = tokens[...].astype(jnp.float32)
    inverse = lax.rsqrt(jnp.mean(values * values, axis=1, keepdims=True) + epsilon)
    columns = pl.ds(pl.multiple_of(t * PART, PART), PART)
    own = (tokens[:, columns].astype(jnp.float32) * inverse * gain[:, columns]).astype(
        jnp.bfloat16
    )
    picks = routes[...]
    raised = jnp.exp(logits[...] - jnp.max(logits[...], axis=0, keepdims=True))
    route_weight = raised / jnp.sum(raised, axis=0, keepdims=True)
    number = lax.broadcasted_iota(jnp.int32, (EXPERTS, TOKENS), 0)
    offset = jnp.where(number % 2 == 1, (number + 1) // 2, (EXPERTS - number // 2) % EXPERTS)
    expert = (me + offset) % EXPERTS
    named = jnp.zeros((EXPERTS, TOKENS), jnp.float32)
    share = jnp.zeros((EXPERTS, TOKENS), jnp.float32)
    for pick in range(4):
        same = picks[pick : pick + 1, :] == expert
        named = named + jnp.where(same, 1.0, 0.0)
        share = share + jnp.where(same, route_weight[pick : pick + 1, :], 0.0)
    before = (
        lax.broadcasted_iota(jnp.int32, (TOKENS, TOKENS), 0)
        < lax.broadcasted_iota(jnp.int32, (TOKENS, TOKENS), 1)
    )
    rank = jnp.dot(
        named.astype(jnp.bfloat16),
        jnp.where(before, 1.0, 0.0).astype(jnp.bfloat16),
        preferred_element_type=jnp.float32,
    )
    slot = jnp.where(named > 0.0, rank, -1.0)
    share_high = share.astype(jnp.bfloat16).astype(jnp.float32)
    share_low = share - share_high
    level = lax.broadcasted_iota(jnp.int32, (SLOTS, TOKENS), 0).astype(jnp.float32)
    for position in range(EXPERTS):
        hit = level == slot[position : position + 1, :]
        rows = slice(position * SLOTS, (position + 1) * SLOTS)
        place[rows, :] = jnp.where(hit, 1.0, 0.0).astype(jnp.bfloat16)
        weigh[0, rows, :] = jnp.where(hit, share_high[position : position + 1, :], 0.0).astype(
            jnp.bfloat16
        )
        weigh[1, rows, :] = jnp.where(hit, share_low[position : position + 1, :], 0.0).astype(
            jnp.bfloat16
        )
    outgoing[...] = jnp.dot(place[...], own, preferred_element_type=jnp.float32).astype(
        jnp.bfloat16
    )
    features[t, 0:SLOTS, :] = outgoing[0:SLOTS, :]
    pl.semaphore_wait(barrier, EXPERTS - 1 + 7)

    started = []

    def send(source, target, send_sem, recv_sem, device):
        copy = pltpu.make_async_remote_copy(
            src_ref=source,
            dst_ref=target,
            send_sem=send_sem[0].at[send_sem[1]],
            recv_sem=recv_sem,
            device_id=device,
            device_id_type=MESH,
        )
        copy.start()
        started.append((source.shape, send_sem))

    def slots(position):
        return pl.ds(position * SLOTS, SLOTS)

    for position in range(1, EXPERTS):
        landing = mirror(position)
        send(
            outgoing.at[slots(position)],
            features.at[t, slots(landing)],
            (go_send, (position,)),
            go_recv.at[landing],
            along(offset_at(position)),
        )

    def rows_of(chunk):
        return pl.ds(chunk * CHUNK, CHUNK)

    def spread(chunk):
        for position in range(chunk * PER_CHUNK, (chunk + 1) * PER_CHUNK):
            if position:
                landed(features.at[t, slots(position)], go_recv.at[position])
        block = features.at[t, rows_of(chunk)]
        for kind, target in ((0, above), (1, below), (4, beside)):
            send(block, block, (ag_send, (chunk, kind,)), ag_recv.at[chunk, kind], {"tp": target})

    def forward(chunk):
        for kind, source, target, first in ((0, below, above, 0), (1, above, below, HALF)):
            block = features.at[source, rows_of(chunk)]
            landed(block, ag_recv.at[chunk, kind])
            part = features.at[source, pl.ds(chunk * CHUNK + first, HALF)]
            send(part, part, (ag_send, (chunk, 2 + kind,)), ag_recv.at[chunk, 2 + kind], {"tp": target})
            send(block, block, (ag_send, (chunk, 5 + kind,)), ag_recv.at[chunk, 5 + kind], {"tp": beside})

    def complete(chunk):
        for kind, first in ((2, 0), (3, HALF)):
            landed(
                features.at[across, pl.ds(chunk * CHUNK + first, HALF)], ag_recv.at[chunk, kind]
            )
        block = features.at[across, rows_of(chunk)]
        send(block, block, (ag_send, (chunk, 7,)), ag_recv.at[chunk, 7], {"tp": beside})

    def multiply(chunk):
        for kind, source in ((4, beside), (5, twin(below)), (6, twin(above)), (7, twin(across))):
            landed(features.at[source, rows_of(chunk)], ag_recv.at[chunk, kind])
        if chunk == 0:
            for load in loads[1:4]:
                load.wait()
        gate_sum = jnp.zeros((CHUNK, PART), jnp.float32)
        up_sum = jnp.zeros((CHUNK, PART), jnp.float32)
        for source in range(8):
            rows = features[source, rows_of(chunk), :]
            depth = slice(source * PART, (source + 1) * PART)
            gate_sum = gate_sum + jnp.dot(rows, gate[depth, :], preferred_element_type=jnp.float32)
            up_sum = up_sum + jnp.dot(rows, up[depth, :], preferred_element_type=jnp.float32)
        gate_cut = jnp.minimum(gate_sum, clamp_limit)
        up_cut = jnp.clip(up_sum, -clamp_limit, clamp_limit)
        hidden = ((up_cut + 1.0) * gate_cut * jax.nn.sigmoid(sigmoid_slope * gate_cut)).astype(
            jnp.bfloat16
        )
        for other in (1, 0):
            for turn in range(4):
                target = ((y + turn) % 4) * 2 + ((1 - core) if other else core)
                partial[chunk, other, turn] = jnp.dot(
                    hidden,
                    down[:, pl.ds(pl.multiple_of(target * PART, PART), PART)],
                    preferred_element_type=jnp.float32,
                ).astype(jnp.bfloat16)
            if other:
                send(
                    partial.at[chunk, 1],
                    paired.at[chunk],
                    (rs_send, (chunk, 0,)),
                    rs_recv.at[chunk, 0],
                    {"tp": beside},
                )

    def added(*values):
        total = values[0].astype(jnp.float32)
        for value in values[1:]:
            total = total + value.astype(jnp.float32)
        return total.astype(jnp.bfloat16)

    def join(chunk):
        landed(paired.at[chunk], rs_recv.at[chunk, 0])
        partial[chunk, 0, 2] = added(partial[chunk, 0, 2], paired[chunk, 2])
        for kind, first, target in ((1, 0, above), (2, HALF, below)):
            send(
                partial.at[chunk, 0, 2, pl.ds(first, HALF)],
                passed.at[chunk, kind - 1],
                (rs_send, (chunk, kind,)),
                rs_recv.at[chunk, kind],
                {"tp": target},
            )
        for turn in (1, 3, 0):
            partial[chunk, 0, turn] = added(partial[chunk, 0, turn], paired[chunk, turn])

    def pass_on(chunk):
        for kind, turn, first, target in ((1, 1, 0, above), (2, 3, HALF, below)):
            landed(passed.at[chunk, kind - 1], rs_recv.at[chunk, kind])
            rows = slice(first, first + HALF)
            partial[chunk, 0, turn, rows] = added(
                partial[chunk, 0, turn, rows], passed[chunk, kind - 1]
            )
            send(
                partial.at[chunk, 0, turn],
                reached.at[chunk, kind - 1],
                (rs_send, (chunk, 2 + kind,)),
                rs_recv.at[chunk, 2 + kind],
                {"tp": target},
            )

    def finish(chunk):
        for kind in (3, 4):
            landed(reached.at[chunk, kind - 3], rs_recv.at[chunk, kind])
        result[rows_of(chunk), :] = added(
            partial[chunk, 0, 0], reached[chunk, 0], reached[chunk, 1]
        )
        for position in range(chunk * PER_CHUNK, (chunk + 1) * PER_CHUNK):
            if position == 0:
                returned[0:SLOTS, :] = result[0:SLOTS, :]
                continue
            landing = mirror(position)
            send(
                result.at[slots(position)],
                returned.at[slots(landing)],
                (back_send, (position,)),
                back_recv.at[landing],
                along(offset_at(position)),
            )

    def plane_of(turn):
        step = (turn + 1) // 2
        return (z + (8 - step if turn % 2 else step)) % PLANES

    def block_of(turn, side):
        return plane_of(turn) * 4 + (x + side) % 4

    a_rows = pl.ds(0, FIRST)
    a_halves = (pl.ds(0, FIRST // 2), pl.ds(FIRST // 2, FIRST // 2))
    b_rows = pl.ds(FIRST, SECOND)
    b_halves = (pl.ds(FIRST, SECOND // 2), pl.ds(FIRST + SECOND // 2, SECOND // 2))
    z_next = ({"ep_0": (z + 1) % PLANES}, {"ep_0": (z + 7) % PLANES})
    x_next = ({"ep_1": (x + 1) % 4}, {"ep_1": (x + 3) % 4})

    def along_x(turn):
        piece = keys.at[block_of(turn, 0), a_rows]
        for way in range(2):
            send(piece, piece, (ax_send, (turn, way,)), ax_recv.at[turn, way], x_next[way])

    def keys_start():
        loads[0].wait()
        piece = keys.at[me, a_rows]
        for way in range(2):
            send(piece, piece, (az_send, (way, 0,)), az_recv.at[way, 0], z_next[way])
        rest = keys.at[me, b_rows]
        for way in range(2):
            send(rest, rest, (bx_send, (way,)), bx_recv.at[way], x_next[way])
        along_x(0)

    def turn_at(step, way):
        return 7 if step == 4 else 2 * step - 1 + way

    def a_z(step):
        for way in range(2):
            block = block_of(turn_at(step, way), 0)
            rows = a_rows if step < 4 else a_halves[way]
            landed(keys.at[block, rows], az_recv.at[way, step - 1])
            if step < 4:
                piece = keys.at[block, a_rows if step < 3 else a_halves[way]]
                send(piece, piece, (az_send, (way, step,)), az_recv.at[way, step], z_next[way])
                along_x(turn_at(step, way))
        if step == 4:
            along_x(7)

    def a_x(turn):
        for way, side in ((0, 3), (1, 1)):
            block = block_of(turn, side)
            landed(keys.at[block, a_rows], ax_recv.at[turn, way])
            piece = keys.at[block, a_halves[way]]
            send(piece, piece, (ax_send, (turn, 2 + way,)), ax_recv.at[turn, 2 + way], x_next[way])

    def a_done(turn):
        for way in range(2):
            landed(keys.at[block_of(turn, 2), a_halves[way]], ax_recv.at[turn, 2 + way])

    def b_x():
        for way, side in ((0, 3), (1, 1)):
            block = block_of(0, side)
            landed(keys.at[block, b_rows], bx_recv.at[way])
            piece = keys.at[block, b_halves[way]]
            send(piece, piece, (bx_send, (2 + way,)), bx_recv.at[2 + way], x_next[way])

    def b_row():
        for way in range(2):
            landed(keys.at[block_of(0, 2), b_halves[way]], bx_recv.at[2 + way])
        pieces = keys.at[pl.ds(z * 4, 4), b_rows]
        for way in range(2):
            send(pieces, pieces, (bz_send, (way, 0,)), bz_recv.at[way, 0], z_next[way])

    def b_z(step):
        for way in range(2):
            blocks = pl.ds(plane_of(turn_at(step, way)) * 4, 4)
            rows = b_rows if step < 4 else b_halves[way]
            landed(keys.at[blocks, rows], bz_recv.at[way, step - 1])
            if step < 4:
                pieces = keys.at[blocks, b_rows if step < 3 else b_halves[way]]
                send(pieces, pieces, (bz_send, (way, step,)), bz_recv.at[way, step], z_next[way])

    start = forget[:, pl.ds(pl.multiple_of(me * ROWS, ROWS), 128)][:, 0:1]

    def key_rows(block):
        gate_rows = pl.ds(pl.multiple_of(block * ROWS, ROWS), ROWS)
        return key_operand(keys[block], forget[:, gate_rows] - start)

    def own_block():
        query_operand(queries[...], qx)
        lanes = key_rows(me)
        values = value_operand(keys[me])
        for tile in range(ASKED // TILE):
            cut = slice(tile * TILE, (tile + 1) * TILE)
            scores = jnp.dot(lanes, qx[:, cut], preferred_element_type=jnp.float32)
            key_at = lax.broadcasted_iota(jnp.int32, (ROWS, TILE), 0)
            query_at = lax.broadcasted_iota(jnp.int32, (ROWS, TILE), 1) + (tile * TILE) % ROWS
            scores = jnp.where(key_at <= query_at, scores, -jnp.inf)
            new = jnp.max(scores, axis=0, keepdims=True)
            weights = jnp.exp(scores - new).astype(jnp.bfloat16)
            acc[:, cut] = jnp.dot(values, weights, preferred_element_type=jnp.float32)
            top[:, cut] = new

    def take(block, after, slot):
        lanes = key_rows(after)
        values = value_operand(keys[block])
        for tile in range(ASKED // TILE):
            cut = slice(tile * TILE, (tile + 1) * TILE)
            s_ref[1 - slot, :, cut] = jnp.dot(
                lanes, qx[:, cut], preferred_element_type=jnp.float32
            )
            scores = s_ref[slot, :, cut]
            old = top[:, cut]
            new = jnp.maximum(old, jnp.max(scores, axis=0, keepdims=True))
            weights = jnp.exp(scores - new).astype(jnp.bfloat16)
            acc[:, cut] = acc[:, cut] * jnp.exp(old - new) + jnp.dot(
                values, weights, preferred_element_type=jnp.float32
            )
            top[:, cut] = new

    def attend(first, count):
        @pl.when(count > 0)
        def _():
            lanes = key_rows(first)
            for tile in range(ASKED // TILE):
                cut = slice(tile * TILE, (tile + 1) * TILE)
                s_ref[0, :, cut] = jnp.dot(
                    lanes, qx[:, cut], preferred_element_type=jnp.float32
                )
            last = first + count - 1

            def pair(step, _):
                block = first + 2 * step
                take(block, jnp.minimum(block + 1, last), 0)

                @pl.when(block + 1 <= last)
                def _():
                    take(block + 1, jnp.minimum(block + 2, last), 1)

                return 0

            lax.fori_loop(0, (count + 1) // 2, pair, 0)

    before_rounds = (
        (keys_start,), (own_block,), (spread, 0), (spread, 1), (forward, 0), (spread, 2),
        (forward, 1), (complete, 0), (spread, 3), (multiply, 0), (forward, 2), (a_z, 1), (b_x,),
        (complete, 1), (join, 0), (multiply, 1), (forward, 3), (a_x, 0), (b_row,), (a_z, 2),
        (complete, 2), (pass_on, 0), (join, 1), (multiply, 2), (a_x, 1), (a_x, 2), (a_z, 3),
        (b_z, 1), (complete, 3), (finish, 0), (pass_on, 1), (join, 2), (multiply, 3),
        (a_done, 0), (a_x, 3), (a_x, 4), (a_z, 4),
    )
    rounds = (
        (),
        ((finish, 1), (pass_on, 2), (join, 3), (a_done, 1), (b_z, 2)),
        ((a_x, 5), (a_x, 6), (a_done, 2)),
        ((finish, 2), (pass_on, 3), (a_x, 7), (a_done, 3)),
        ((a_done, 4), (b_z, 3)),
        ((finish, 3), (a_done, 5)),
        ((a_done, 6), (b_z, 4)),
        ((a_done, 7),),
    )

    for step, *at in before_rounds:
        step(*at)

    def one_round(turn, _):
        for number, events in enumerate(rounds):
            if events:

                @pl.when(turn == number)
                def _(events=events):
                    for step, *at in events:
                        step(*at)

        odd = turn % 2
        step = (turn + 1) // 2
        plane = jnp.where(odd == 1, z - step, z + step - jnp.where(turn > 0, PLANES, 0))
        count = jnp.where(turn == 0, x, jnp.where(plane >= 0, 4, 0))
        attend(jnp.maximum(plane, 0) * 4, count)
        return 0

    lax.fori_loop(0, PLANES, one_round, 0)

    total = acc[...]
    heads = total[0:HEAD] / total[HEAD : HEAD + 1]
    both = jnp.concatenate([heads[:, 0:ROWS], heads[:, ROWS:ASKED]], axis=0)
    attended[...] = both.T.astype(jnp.bfloat16)
    for offset in range(1, 8):
        peer = (t + offset) % 8
        send(
            attended.at[pl.ds(pl.multiple_of(peer * SHARE, SHARE), SHARE)],
            gathered.at[t],
            (at_send, (offset,)),
            at_recv.at[8 - offset],
            {"tp": peer},
        )
    gathered[t] = attended[pl.ds(pl.multiple_of(t * SHARE, SHARE), SHARE), :]

    for position in range(1, EXPERTS):
        landed(returned.at[slots(position)], back_recv.at[position])
    turned = (((0,), (0,)), ((), ()))
    out[...] = (
        lax.dot_general(weigh[0], returned[...], turned, preferred_element_type=jnp.float32)
        + lax.dot_general(weigh[1], returned[...], turned, preferred_element_type=jnp.float32)
    ).astype(jnp.bfloat16)

    loads[4].wait()
    for offset in range(1, 8):
        landed(gathered.at[(t + offset) % 8], at_recv.at[offset])
    rows = jnp.concatenate([gathered[source] for source in range(8)], axis=1).astype(jnp.float32)
    inverse = lax.rsqrt(jnp.mean(rows * rows, axis=1, keepdims=True) + epsilon)
    normed = (rows * inverse * heads_gain[...]).astype(jnp.bfloat16)
    mixer_out[...] = jnp.dot(normed, mix[...], preferred_element_type=jnp.float32).astype(
        jnp.bfloat16
    )

    for shape, sem in started:
        if shape[-1] == PART:
            room = partial.at[0, 0] if len(shape) == 3 else returned.at[pl.ds(0, shape[0])]
        elif len(shape) == 3:
            room = keys.at[pl.ds(0, 4), pl.ds(0, shape[1])]
        else:
            room = keys.at[0, pl.ds(0, shape[0])]
        landed(room, sem[0].at[sem[1]])


def body(
    queries,
    keys_values,
    forget_cache,
    heads_gain,
    output_weight,
    expert_tokens,
    expert_gain,
    routes,
    route_logits,
    gate_weight,
    up_weight,
    down_weight,
):
    vmem = pl.BlockSpec(memory_space=pltpu.VMEM)
    anywhere = pl.BlockSpec(memory_space=pl.ANY)
    half = jnp.bfloat16
    dma = pltpu.SemaphoreType.DMA
    moe_out, mixer_out = pl.pallas_call(
        kernel,
        out_shape=(
            jax.ShapeDtypeStruct((TOKENS, PART), half),
            jax.ShapeDtypeStruct((SHARE, WIDTH), half),
        ),
        in_specs=[vmem] * 4 + [anywhere] * 3 + [vmem] * 3 + [anywhere] * 2,
        out_specs=(vmem, vmem),
        scratch_shapes=[
            pltpu.VMEM((WIDTH, PART), half),
            pltpu.VMEM((WIDTH, PART), half),
            pltpu.VMEM((PART, WIDTH), half),
            pltpu.VMEM((ALL_SLOTS, TOKENS), half),
            pltpu.VMEM((2, ALL_SLOTS, TOKENS), half),
            pltpu.VMEM((ALL_SLOTS, PART), half),
            pltpu.VMEM((8, ALL_SLOTS, PART), half),
            pltpu.VMEM((CHUNKS, 2, 4, CHUNK, PART), half),
            pltpu.VMEM((CHUNKS, 4, CHUNK, PART), half),
            pltpu.VMEM((CHUNKS, 2, HALF, PART), half),
            pltpu.VMEM((CHUNKS, 2, CHUNK, PART), half),
            pltpu.VMEM((ALL_SLOTS, PART), half),
            pltpu.VMEM((ALL_SLOTS, PART), half),
            pltpu.VMEM((16 * HEAD, WIDTH), half),
            pltpu.VMEM((4 * PLANES, ROWS, 2 * HEAD), half),
            pltpu.VMEM((2 * HEAD, ASKED), half),
            pltpu.VMEM((1, ASKED), jnp.float32),
            pltpu.VMEM((HEAD + 16, ASKED), jnp.float32),
            pltpu.VMEM((2, ROWS, ASKED), jnp.float32),
            pltpu.VMEM((ROWS, 2 * HEAD), half),
            pltpu.VMEM((8, SHARE, 2 * HEAD), half),
            dma((5,)),
            dma((EXPERTS,)),
            dma((EXPERTS,)),
            dma((CHUNKS, 8)),
            dma((CHUNKS, 8)),
            dma((CHUNKS, 5)),
            dma((CHUNKS, 5)),
            dma((EXPERTS,)),
            dma((EXPERTS,)),
            dma((2, 4)),
            dma((2, 4)),
            dma((PLANES, 4)),
            dma((PLANES, 4)),
            dma((4,)),
            dma((4,)),
            dma((2, 4)),
            dma((2, 4)),
            dma((8,)),
            dma((8,)),
        ],
        compiler_params=pltpu.CompilerParams(
            collective_id=0, has_side_effects=True, vmem_limit_bytes=60 * 2**20
        ),
    )(
        expert_tokens,
        expert_gain.reshape(1, -1),
        routes.T,
        route_logits.T,
        gate_weight[0],
        up_weight[0],
        down_weight[0],
        queries,
        forget_cache,
        heads_gain.reshape(1, -1),
        keys_values,
        output_weight,
    )
    return (mixer_out, moe_out)


def solution(mesh):
    torus = Mesh(mesh.devices.reshape(8, 4, mesh.shape["tp"]), ("ep_0", "ep_1", "tp"))
    return jax.shard_map(
        body,
        mesh=torus,
        in_specs=(
            P(EP, "tp"),
            P(EP, "tp"),
            P("tp", None),
            P(),
            P(),
            P(EP, None),
            P(),
            P(EP, None),
            P(EP, None),
            P(EP, None, "tp"),
            P(EP, None, "tp"),
            P(EP, "tp", None),
        ),
        out_specs=(P(EP_TP, None), P(EP, "tp")),
        check_vma=False,
    )
```

```python
import math

import jax
import jax.numpy as jnp
from jax import lax
from jax.experimental import pallas as pl
from jax.experimental.pallas import tpu as pltpu
from jax.sharding import Mesh
from jax.sharding import PartitionSpec as P

HEAD = 64
EP = ("ep_0", "ep_1")
EP_TP = ("ep_0", "ep_1", "tp")


epsilon = 1e-06
clamp_limit = 7.0
sigmoid_slope = 1.702


def split3(x):
    hi = x.astype(jnp.bfloat16)
    rest = x - hi.astype(jnp.float32)
    mid = rest.astype(jnp.bfloat16)
    low = (rest - mid.astype(jnp.float32)).astype(jnp.bfloat16)
    return hi, mid, low


ROWS = 512
ASKED = 2 * ROWS
TILE = 256


def query_operand(query_rows, qx):
    turned = (query_rows.astype(jnp.float32) * (1.0 / math.sqrt(HEAD))).T.astype(jnp.bfloat16)
    row = lax.broadcasted_iota(jnp.int32, (HEAD, ASKED), 0)
    col = lax.broadcasted_iota(jnp.int32, (HEAD, ASKED), 1)
    first = (col < ROWS) & (row < 3)
    second = (col >= ROWS) & (row >= 3) & (row < 6)
    qx[0:HEAD, 0:ROWS] = turned[0:HEAD]
    qx[0:HEAD, ROWS:ASKED] = turned[HEAD : 2 * HEAD]
    qx[HEAD : 2 * HEAD, :] = jnp.where(first | second, -1.0, 0.0).astype(jnp.bfloat16)


def key_operand(block_rows, gate):
    hi, mid, low = split3(gate)
    parts = jnp.concatenate(
        [hi[0:1], mid[0:1], low[0:1], hi[1:2], mid[1:2], low[1:2]], axis=0
    ).astype(jnp.float32)
    full = jnp.concatenate(
        [jnp.zeros((64, ROWS), jnp.float32), parts, jnp.zeros((58, ROWS), jnp.float32)], axis=0
    )
    lane = lax.broadcasted_iota(jnp.int32, (ROWS, 2 * HEAD), 1)
    return jnp.where(lane < HEAD, block_rows, full.T.astype(jnp.bfloat16))


def value_operand(block_rows):
    turned = block_rows.astype(jnp.float32).T[HEAD : 2 * HEAD].astype(jnp.bfloat16)
    return jnp.concatenate([turned, jnp.ones((16, ROWS), jnp.bfloat16)], axis=0)


MESH = pl.DeviceIdType.MESH
EXPERTS = 32
SLOTS = 32
TOKENS = 128
WIDTH = 2048
PART = 256
ALL_SLOTS = EXPERTS * SLOTS
CHUNKS = 4
CHUNK = ALL_SLOTS // CHUNKS
PER_CHUNK = CHUNK // SLOTS
HALF = CHUNK // 2
PLANES = 8
FIRST = 320
SECOND = ROWS - FIRST
SHARE = ROWS // 8


def offset_at(position):
    return (position + 1) // 2 if position % 2 else (EXPERTS - position // 2) % EXPERTS


def mirror(position):
    if position in (0, EXPERTS - 1):
        return position
    return position + 1 if position % 2 else position - 1


def landed(ref, sem):
    pltpu.make_async_copy(ref, ref, sem).wait()


def kernel(
    tokens,
    gain,
    routes,
    logits,
    gate_hbm,
    up_hbm,
    down_hbm,
    queries,
    forget,
    heads_gain,
    own_hbm,
    mix_hbm,
    out,
    mixer_out,
    gate,
    up,
    down,
    place,
    weigh,
    outgoing,
    features,
    partial,
    paired,
    passed,
    reached,
    result,
    returned,
    mix,
    keys,
    qx,
    top,
    acc,
    s_ref,
    attended,
    gathered,
    load_sem,
    sent,
    go_recv,
    ag_recv,
    rs_recv,
    back_recv,
    az_recv,
    ax_recv,
    bx_recv,
    bz_recv,
    at_recv,
):
    z, x, t = lax.axis_index("ep_0"), lax.axis_index("ep_1"), lax.axis_index("tp")
    me = z * 4 + x
    y, core = t // 2, t % 2
    above = ((y + 1) % 4) * 2 + core
    below = ((y + 3) % 4) * 2 + core
    across = ((y + 2) % 4) * 2 + core
    beside = y * 2 + (1 - core)

    def twin(number):
        return (number // 2) * 2 + 1 - core

    def along(offset):
        peer = (me + offset) % EXPERTS
        return {"ep_0": peer // 4, "ep_1": peer % 4}

    barrier = pltpu.get_barrier_semaphore()
    for offset in range(1, EXPERTS):
        pl.semaphore_signal(barrier, inc=1, device_id=along(offset), device_id_type=MESH)
    for offset in range(1, 8):
        pl.semaphore_signal(
            barrier, inc=1, device_id={"tp": (t + offset) % 8}, device_id_type=MESH
        )
    loads = [
        pltpu.make_async_copy(source, target, load_sem.at[number])
        for number, (source, target) in enumerate(
            (
                (own_hbm, keys.at[me]),
                (gate_hbm, gate),
                (up_hbm, up),
                (down_hbm, down),
                (mix_hbm, mix),
            )
        )
    ]
    for load in loads:
        load.start()

    values = tokens[...].astype(jnp.float32)
    inverse = lax.rsqrt(jnp.mean(values * values, axis=1, keepdims=True) + epsilon)
    columns = pl.ds(pl.multiple_of(t * PART, PART), PART)
    own = (tokens[:, columns].astype(jnp.float32) * inverse * gain[:, columns]).astype(
        jnp.bfloat16
    )
    picks = routes[...]
    raised = jnp.exp(logits[...] - jnp.max(logits[...], axis=0, keepdims=True))
    route_weight = raised / jnp.sum(raised, axis=0, keepdims=True)
    number = lax.broadcasted_iota(jnp.int32, (EXPERTS, TOKENS), 0)
    offset = jnp.where(number % 2 == 1, (number + 1) // 2, (EXPERTS - number // 2) % EXPERTS)
    expert = (me + offset) % EXPERTS
    named = jnp.zeros((EXPERTS, TOKENS), jnp.float32)
    share = jnp.zeros((EXPERTS, TOKENS), jnp.float32)
    for pick in range(4):
        same = picks[pick : pick + 1, :] == expert
        named = named + jnp.where(same, 1.0, 0.0)
        share = share + jnp.where(same, route_weight[pick : pick + 1, :], 0.0)
    before = (
        lax.broadcasted_iota(jnp.int32, (TOKENS, TOKENS), 0)
        < lax.broadcasted_iota(jnp.int32, (TOKENS, TOKENS), 1)
    )
    rank = jnp.dot(
        named.astype(jnp.bfloat16),
        jnp.where(before, 1.0, 0.0).astype(jnp.bfloat16),
        preferred_element_type=jnp.float32,
    )
    slot = jnp.where(named > 0.0, rank, -1.0)
    share_high = share.astype(jnp.bfloat16).astype(jnp.float32)
    share_low = share - share_high
    level = lax.broadcasted_iota(jnp.int32, (SLOTS, TOKENS), 0).astype(jnp.float32)
    for position in range(EXPERTS):
        hit = level == slot[position : position + 1, :]
        rows = slice(position * SLOTS, (position + 1) * SLOTS)
        place[rows, :] = jnp.where(hit, 1.0, 0.0).astype(jnp.bfloat16)
        weigh[0, rows, :] = jnp.where(hit, share_high[position : position + 1, :], 0.0).astype(
            jnp.bfloat16
        )
        weigh[1, rows, :] = jnp.where(hit, share_low[position : position + 1, :], 0.0).astype(
            jnp.bfloat16
        )
    outgoing[...] = jnp.dot(place[...], own, preferred_element_type=jnp.float32).astype(
        jnp.bfloat16
    )
    features[t, 0:SLOTS, :] = outgoing[0:SLOTS, :]
    pl.semaphore_wait(barrier, EXPERTS - 1 + 7)

    def send(source, target, send_sem, recv_sem, device):
        copy = pltpu.make_async_remote_copy(
            src_ref=source,
            dst_ref=target,
            send_sem=send_sem,
            recv_sem=recv_sem,
            device_id=device,
            device_id_type=MESH,
        )
        copy.start()

    def slots(position):
        return pl.ds(position * SLOTS, SLOTS)

    for position in range(1, EXPERTS):
        landing = mirror(position)
        send(
            outgoing.at[slots(position)],
            features.at[t, slots(landing)],
            sent.at[0],
            go_recv.at[landing // PER_CHUNK],
            along(offset_at(position)),
        )

    def rows_of(chunk):
        return pl.ds(chunk * CHUNK, CHUNK)

    def spread(chunk):
        first = SLOTS if chunk == 0 else 0
        landed(
            features.at[t, pl.ds(chunk * CHUNK + first, CHUNK - first)], go_recv.at[chunk]
        )
        block = features.at[t, rows_of(chunk)]
        for kind, target in ((0, above), (1, below), (3, beside)):
            send(block, block, sent.at[1], ag_recv.at[chunk, kind], {"tp": target})

    def forward(chunk):
        for kind, source, target, first in ((0, below, above, 0), (1, above, below, HALF)):
            block = features.at[source, rows_of(chunk)]
            landed(block, ag_recv.at[chunk, kind])
            part = features.at[source, pl.ds(chunk * CHUNK + first, HALF)]
            send(part, part, sent.at[1], ag_recv.at[chunk, 2], {"tp": target})
            send(block, block, sent.at[1], ag_recv.at[chunk, 3], {"tp": beside})

    def complete(chunk):
        block = features.at[across, rows_of(chunk)]
        landed(block, ag_recv.at[chunk, 2])
        send(block, block, sent.at[1], ag_recv.at[chunk, 3], {"tp": beside})

    def multiply(chunk):
        landed(features.at[pl.ds(0, 4), rows_of(chunk)], ag_recv.at[chunk, 3])
        if chunk == 0:
            for load in loads[1:4]:
                load.wait()
        gate_sum = jnp.zeros((CHUNK, PART), jnp.float32)
        up_sum = jnp.zeros((CHUNK, PART), jnp.float32)
        for source in range(8):
            rows = features[source, rows_of(chunk), :]
            depth = slice(source * PART, (source + 1) * PART)
            gate_sum = gate_sum + jnp.dot(rows, gate[depth, :], preferred_element_type=jnp.float32)
            up_sum = up_sum + jnp.dot(rows, up[depth, :], preferred_element_type=jnp.float32)
        gate_cut = jnp.minimum(gate_sum, clamp_limit)
        up_cut = jnp.clip(up_sum, -clamp_limit, clamp_limit)
        hidden = ((up_cut + 1.0) * gate_cut * jax.nn.sigmoid(sigmoid_slope * gate_cut)).astype(
            jnp.bfloat16
        )
        for other in (1, 0):
            for turn in range(4):
                target = ((y + turn) % 4) * 2 + ((1 - core) if other else core)
                partial[chunk, other, turn] = jnp.dot(
                    hidden,
                    down[:, pl.ds(pl.multiple_of(target * PART, PART), PART)],
                    preferred_element_type=jnp.float32,
                ).astype(jnp.bfloat16)
            if other:
                send(
                    partial.at[chunk, 1],
                    paired.at[chunk],
                    sent.at[2],
                    rs_recv.at[chunk, 0],
                    {"tp": beside},
                )

    def added(*values):
        total = values[0].astype(jnp.float32)
        for value in values[1:]:
            total = total + value.astype(jnp.float32)
        return total.astype(jnp.bfloat16)

    def join(chunk):
        landed(paired.at[chunk], rs_recv.at[chunk, 0])
        partial[chunk, 0, 2] = added(partial[chunk, 0, 2], paired[chunk, 2])
        for kind, first, target in ((1, 0, above), (2, HALF, below)):
            send(
                partial.at[chunk, 0, 2, pl.ds(first, HALF)],
                passed.at[chunk, kind - 1],
                sent.at[2],
                rs_recv.at[chunk, kind],
                {"tp": target},
            )
        for turn in (1, 3, 0):
            partial[chunk, 0, turn] = added(partial[chunk, 0, turn], paired[chunk, turn])

    def pass_on(chunk):
        for kind, turn, first, target in ((1, 1, 0, above), (2, 3, HALF, below)):
            landed(passed.at[chunk, kind - 1], rs_recv.at[chunk, kind])
            rows = slice(first, first + HALF)
            partial[chunk, 0, turn, rows] = added(
                partial[chunk, 0, turn, rows], passed[chunk, kind - 1]
            )
            send(
                partial.at[chunk, 0, turn],
                reached.at[chunk, kind - 1],
                sent.at[2],
                rs_recv.at[chunk, 3],
                {"tp": target},
            )

    def finish(chunk):
        landed(reached.at[chunk], rs_recv.at[chunk, 3])
        result[rows_of(chunk), :] = added(
            partial[chunk, 0, 0], reached[chunk, 0], reached[chunk, 1]
        )
        for position in range(chunk * PER_CHUNK, (chunk + 1) * PER_CHUNK):
            if position == 0:
                returned[0:SLOTS, :] = result[0:SLOTS, :]
                continue
            landing = mirror(position)
            send(
                result.at[slots(position)],
                returned.at[slots(landing)],
                sent.at[3],
                back_recv.at[0],
                along(offset_at(position)),
            )

    def plane_of(turn):
        step = (turn + 1) // 2
        return (z + (8 - step if turn % 2 else step)) % PLANES

    def block_of(turn, side):
        return plane_of(turn) * 4 + (x + side) % 4

    a_rows = pl.ds(0, FIRST)
    a_halves = (pl.ds(0, FIRST // 2), pl.ds(FIRST // 2, FIRST // 2))
    b_rows = pl.ds(FIRST, SECOND)
    b_halves = (pl.ds(FIRST, SECOND // 2), pl.ds(FIRST + SECOND // 2, SECOND // 2))
    z_next = ({"ep_0": (z + 1) % PLANES}, {"ep_0": (z + 7) % PLANES})
    x_next = ({"ep_1": (x + 1) % 4}, {"ep_1": (x + 3) % 4})

    def along_x(turn):
        piece = keys.at[block_of(turn, 0), a_rows]
        for way in range(2):
            send(piece, piece, sent.at[4], ax_recv.at[turn, way], x_next[way])

    def keys_start():
        loads[0].wait()
        piece = keys.at[me, a_rows]
        for way in range(2):
            send(piece, piece, sent.at[4], az_recv.at[way, 0], z_next[way])
        rest = keys.at[me, b_rows]
        for way in range(2):
            send(rest, rest, sent.at[4], bx_recv.at[way], x_next[way])
        along_x(0)

    def turn_at(step, way):
        return 7 if step == 4 else 2 * step - 1 + way

    def a_z(step):
        for way in range(2):
            block = block_of(turn_at(step, way), 0)
            rows = a_rows if step < 4 else a_halves[way]
            landed(keys.at[block, rows], az_recv.at[way, step - 1])
            if step < 4:
                piece = keys.at[block, a_rows if step < 3 else a_halves[way]]
                send(piece, piece, sent.at[4], az_recv.at[way, step], z_next[way])
                along_x(turn_at(step, way))
        if step == 4:
            along_x(7)

    def a_x(turn):
        for way, side in ((0, 3), (1, 1)):
            block = block_of(turn, side)
            landed(keys.at[block, a_rows], ax_recv.at[turn, way])
            piece = keys.at[block, a_halves[way]]
            send(piece, piece, sent.at[4], ax_recv.at[turn, 2], x_next[way])

    def a_done(turn):
        landed(keys.at[block_of(turn, 2), a_rows], ax_recv.at[turn, 2])

    def b_x():
        for way, side in ((0, 3), (1, 1)):
            block = block_of(0, side)
            landed(keys.at[block, b_rows], bx_recv.at[way])
            piece = keys.at[block, b_halves[way]]
            send(piece, piece, sent.at[4], bx_recv.at[2], x_next[way])

    def b_row():
        landed(keys.at[block_of(0, 2), b_rows], bx_recv.at[2])
        pieces = keys.at[pl.ds(z * 4, 4), b_rows]
        for way in range(2):
            send(pieces, pieces, sent.at[4], bz_recv.at[way, 0], z_next[way])

    def b_z(step):
        for way in range(2):
            blocks = pl.ds(plane_of(turn_at(step, way)) * 4, 4)
            rows = b_rows if step < 4 else b_halves[way]
            landed(keys.at[blocks, rows], bz_recv.at[way, step - 1])
            if step < 4:
                pieces = keys.at[blocks, b_rows if step < 3 else b_halves[way]]
                send(pieces, pieces, sent.at[4], bz_recv.at[way, step], z_next[way])

    start = forget[:, pl.ds(pl.multiple_of(me * ROWS, ROWS), 128)][:, 0:1]

    def key_rows(block):
        gate_rows = pl.ds(pl.multiple_of(block * ROWS, ROWS), ROWS)
        return key_operand(keys[block], forget[:, gate_rows] - start)

    def own_block():
        query_operand(queries[...], qx)
        lanes = key_rows(me)
        values = value_operand(keys[me])
        for tile in range(ASKED // TILE):
            cut = slice(tile * TILE, (tile + 1) * TILE)
            scores = jnp.dot(lanes, qx[:, cut], preferred_element_type=jnp.float32)
            key_at = lax.broadcasted_iota(jnp.int32, (ROWS, TILE), 0)
            query_at = lax.broadcasted_iota(jnp.int32, (ROWS, TILE), 1) + (tile * TILE) % ROWS
            scores = jnp.where(key_at <= query_at, scores, -jnp.inf)
            new = jnp.max(scores, axis=0, keepdims=True)
            weights = jnp.exp(scores - new).astype(jnp.bfloat16)
            acc[:, cut] = jnp.dot(values, weights, preferred_element_type=jnp.float32)
            top[:, cut] = new

    def take(block, after, slot):
        lanes = key_rows(after)
        values = value_operand(keys[block])
        for tile in range(ASKED // TILE):
            cut = slice(tile * TILE, (tile + 1) * TILE)
            s_ref[1 - slot, :, cut] = jnp.dot(
                lanes, qx[:, cut], preferred_element_type=jnp.float32
            )
            scores = s_ref[slot, :, cut]
            old = top[:, cut]
            new = jnp.maximum(old, jnp.max(scores, axis=0, keepdims=True))
            weights = jnp.exp(scores - new).astype(jnp.bfloat16)
            acc[:, cut] = acc[:, cut] * jnp.exp(old - new) + jnp.dot(
                values, weights, preferred_element_type=jnp.float32
            )
            top[:, cut] = new

    def attend(first, count):
        @pl.when(count > 0)
        def _():
            lanes = key_rows(first)
            for tile in range(ASKED // TILE):
                cut = slice(tile * TILE, (tile + 1) * TILE)
                s_ref[0, :, cut] = jnp.dot(
                    lanes, qx[:, cut], preferred_element_type=jnp.float32
                )
            last = first + count - 1

            def pair(step, _):
                block = first + 2 * step
                take(block, jnp.minimum(block + 1, last), 0)

                @pl.when(block + 1 <= last)
                def _():
                    take(block + 1, jnp.minimum(block + 2, last), 1)

                return 0

            lax.fori_loop(0, (count + 1) // 2, pair, 0)

    before_rounds = (
        (keys_start,), (own_block,), (spread, 0), (spread, 1), (forward, 0), (b_x,), (a_x, 0),
        (spread, 2), (forward, 1), (complete, 0), (a_z, 1), (b_row,), (spread, 3), (a_done, 0),
        (a_x, 1), (a_x, 2), (forward, 2), (complete, 1),
    )
    rounds = (
        (),
        ((a_z, 2), (b_z, 1), (multiply, 0), (a_done, 1), (a_done, 2)),
        (
            (join, 0), (forward, 3), (complete, 2), (a_x, 3), (a_x, 4), (a_z, 3), (multiply, 1),
        ),
        (
            (join, 1), (pass_on, 0), (b_z, 2), (a_x, 5), (a_x, 6), (complete, 3), (a_z, 4),
            (multiply, 2), (a_done, 3),
        ),
        ((pass_on, 1), (finish, 0), (join, 2), (multiply, 3), (a_x, 7), (a_done, 4)),
        ((b_z, 3), (join, 3), (pass_on, 2), (finish, 1), (a_done, 5)),
        ((pass_on, 3), (finish, 2), (a_done, 6)),
        ((b_z, 4), (finish, 3), (a_done, 7)),
    )

    for step, *at in before_rounds:
        step(*at)

    def one_round(turn, _):
        for number, events in enumerate(rounds):
            if events:

                @pl.when(turn == number)
                def _(events=events):
                    for step, *at in events:
                        step(*at)

        odd = turn % 2
        step = (turn + 1) // 2
        plane = jnp.where(odd == 1, z - step, z + step - jnp.where(turn > 0, PLANES, 0))
        count = jnp.where(turn == 0, x, jnp.where(plane >= 0, 4, 0))
        attend(jnp.maximum(plane, 0) * 4, count)
        return 0

    lax.fori_loop(0, PLANES, one_round, 0)

    total = acc[...]
    heads = total[0:HEAD] / total[HEAD : HEAD + 1]
    both = jnp.concatenate([heads[:, 0:ROWS], heads[:, ROWS:ASKED]], axis=0)
    attended[...] = both.T.astype(jnp.bfloat16)
    for offset in range(1, 8):
        peer = (t + offset) % 8
        send(
            attended.at[pl.ds(pl.multiple_of(peer * SHARE, SHARE), SHARE)],
            gathered.at[t],
            sent.at[5],
            at_recv.at[0],
            {"tp": peer},
        )
    gathered[t] = attended[pl.ds(pl.multiple_of(t * SHARE, SHARE), SHARE), :]

    landed(returned.at[pl.ds(SLOTS, ALL_SLOTS - SLOTS)], back_recv.at[0])
    turned = (((0,), (0,)), ((), ()))
    out[...] = (
        lax.dot_general(weigh[0], returned[...], turned, preferred_element_type=jnp.float32)
        + lax.dot_general(weigh[1], returned[...], turned, preferred_element_type=jnp.float32)
    ).astype(jnp.bfloat16)

    loads[4].wait()
    landed(gathered.at[pl.ds(0, 7)], at_recv.at[0])
    rows = jnp.concatenate([gathered[source] for source in range(8)], axis=1).astype(jnp.float32)
    inverse = lax.rsqrt(jnp.mean(rows * rows, axis=1, keepdims=True) + epsilon)
    normed = (rows * inverse * heads_gain[...]).astype(jnp.bfloat16)
    mixer_out[...] = jnp.dot(normed, mix[...], preferred_element_type=jnp.float32).astype(
        jnp.bfloat16
    )

    rest = pl.ds(0, ALL_SLOTS - SLOTS)
    landed(outgoing.at[rest], sent.at[0])
    landed(features.at[pl.ds(0, 7)], sent.at[1])
    landed(features.at[pl.ds(0, 7)], sent.at[2])
    landed(result.at[rest], sent.at[3])
    landed(keys.at[pl.ds(0, EXPERTS - 1)], sent.at[4])
    landed(gathered.at[pl.ds(0, 7)], sent.at[5])


def body(
    queries,
    keys_values,
    forget_cache,
    heads_gain,
    output_weight,
    expert_tokens,
    expert_gain,
    routes,
    route_logits,
    gate_weight,
    up_weight,
    down_weight,
):
    vmem = pl.BlockSpec(memory_space=pltpu.VMEM)
    anywhere = pl.BlockSpec(memory_space=pl.ANY)
    half = jnp.bfloat16
    dma = pltpu.SemaphoreType.DMA
    moe_out, mixer_out = pl.pallas_call(
        kernel,
        out_shape=(
            jax.ShapeDtypeStruct((TOKENS, PART), half),
            jax.ShapeDtypeStruct((SHARE, WIDTH), half),
        ),
        in_specs=[vmem] * 4 + [anywhere] * 3 + [vmem] * 3 + [anywhere] * 2,
        out_specs=(vmem, vmem),
        scratch_shapes=[
            pltpu.VMEM((WIDTH, PART), half),
            pltpu.VMEM((WIDTH, PART), half),
            pltpu.VMEM((PART, WIDTH), half),
            pltpu.VMEM((ALL_SLOTS, TOKENS), half),
            pltpu.VMEM((2, ALL_SLOTS, TOKENS), half),
            pltpu.VMEM((ALL_SLOTS, PART), half),
            pltpu.VMEM((8, ALL_SLOTS, PART), half),
            pltpu.VMEM((CHUNKS, 2, 4, CHUNK, PART), half),
            pltpu.VMEM((CHUNKS, 4, CHUNK, PART), half),
            pltpu.VMEM((CHUNKS, 2, HALF, PART), half),
            pltpu.VMEM((CHUNKS, 2, CHUNK, PART), half),
            pltpu.VMEM((ALL_SLOTS, PART), half),
            pltpu.VMEM((ALL_SLOTS, PART), half),
            pltpu.VMEM((16 * HEAD, WIDTH), half),
            pltpu.VMEM((4 * PLANES, ROWS, 2 * HEAD), half),
            pltpu.VMEM((2 * HEAD, ASKED), half),
            pltpu.VMEM((1, ASKED), jnp.float32),
            pltpu.VMEM((HEAD + 16, ASKED), jnp.float32),
            pltpu.VMEM((2, ROWS, ASKED), jnp.float32),
            pltpu.VMEM((ROWS, 2 * HEAD), half),
            pltpu.VMEM((8, SHARE, 2 * HEAD), half),
            dma((5,)),
            dma((6,)),
            dma((CHUNKS,)),
            dma((CHUNKS, 4)),
            dma((CHUNKS, 4)),
            dma((1,)),
            dma((2, 4)),
            dma((PLANES, 3)),
            dma((3,)),
            dma((2, 4)),
            dma((1,)),
        ],
        compiler_params=pltpu.CompilerParams(
            collective_id=0, has_side_effects=True, vmem_limit_bytes=60 * 2**20
        ),
    )(
        expert_tokens,
        expert_gain.reshape(1, -1),
        routes.T,
        route_logits.T,
        gate_weight[0],
        up_weight[0],
        down_weight[0],
        queries,
        forget_cache,
        heads_gain.reshape(1, -1),
        keys_values,
        output_weight,
    )
    return (mixer_out, moe_out)


def solution(mesh):
    torus = Mesh(mesh.devices.reshape(8, 4, mesh.shape["tp"]), ("ep_0", "ep_1", "tp"))
    return jax.shard_map(
        body,
        mesh=torus,
        in_specs=(
            P(EP, "tp"),
            P(EP, "tp"),
            P("tp", None),
            P(),
            P(),
            P(EP, None),
            P(),
            P(EP, None),
            P(EP, None),
            P(EP, None, "tp"),
            P(EP, None, "tp"),
            P(EP, "tp", None),
        ),
        out_specs=(P(EP_TP, None), P(EP, "tp")),
        check_vma=False,
    )
```

```python
import math

import jax
import jax.numpy as jnp
from jax import lax
from jax.experimental import pallas as pl
from jax.experimental.pallas import tpu as pltpu
from jax.sharding import Mesh
from jax.sharding import PartitionSpec as P

HEAD = 64
EP = ("ep_0", "ep_1")
EP_TP = ("ep_0", "ep_1", "tp")


epsilon = 1e-06
clamp_limit = 7.0
sigmoid_slope = 1.702


def split3(x):
    hi = x.astype(jnp.bfloat16)
    rest = x - hi.astype(jnp.float32)
    mid = rest.astype(jnp.bfloat16)
    low = (rest - mid.astype(jnp.float32)).astype(jnp.bfloat16)
    return hi, mid, low


ROWS = 512
ASKED = 2 * ROWS
TILE = 256


def query_operand(query_rows, qx):
    turned = (query_rows.astype(jnp.float32) * (1.0 / math.sqrt(HEAD))).T.astype(jnp.bfloat16)
    row = lax.broadcasted_iota(jnp.int32, (HEAD, ASKED), 0)
    col = lax.broadcasted_iota(jnp.int32, (HEAD, ASKED), 1)
    first = (col < ROWS) & (row < 3)
    second = (col >= ROWS) & (row >= 3) & (row < 6)
    qx[0:HEAD, 0:ROWS] = turned[0:HEAD]
    qx[0:HEAD, ROWS:ASKED] = turned[HEAD : 2 * HEAD]
    qx[HEAD : 2 * HEAD, :] = jnp.where(first | second, -1.0, 0.0).astype(jnp.bfloat16)


def key_operand(block_rows, gate):
    hi, mid, low = split3(gate)
    parts = jnp.concatenate(
        [hi[0:1], mid[0:1], low[0:1], hi[1:2], mid[1:2], low[1:2]], axis=0
    ).astype(jnp.float32)
    full = jnp.concatenate(
        [jnp.zeros((64, ROWS), jnp.float32), parts, jnp.zeros((58, ROWS), jnp.float32)], axis=0
    )
    lane = lax.broadcasted_iota(jnp.int32, (ROWS, 2 * HEAD), 1)
    return jnp.where(lane < HEAD, block_rows, full.T.astype(jnp.bfloat16))


def value_operand(block_rows):
    turned = block_rows.astype(jnp.float32).T[HEAD : 2 * HEAD].astype(jnp.bfloat16)
    return jnp.concatenate([turned, jnp.ones((16, ROWS), jnp.bfloat16)], axis=0)


MESH = pl.DeviceIdType.MESH
EXPERTS = 32
SLOTS = 32
TOKENS = 128
WIDTH = 2048
PART = 256
ALL_SLOTS = EXPERTS * SLOTS
CHUNKS = 4
CHUNK = ALL_SLOTS // CHUNKS
PER_CHUNK = CHUNK // SLOTS
HALF = CHUNK // 2
PLANES = 8
FIRST = 320
SECOND = ROWS - FIRST
SHARE = ROWS // 8


def offset_at(position):
    return (position + 1) // 2 if position % 2 else (EXPERTS - position // 2) % EXPERTS


def mirror(position):
    if position in (0, EXPERTS - 1):
        return position
    return position + 1 if position % 2 else position - 1


def landed(ref, sem):
    pltpu.make_async_copy(ref, ref, sem).wait()


def kernel(
    tokens,
    gain,
    routes,
    logits,
    gate_hbm,
    up_hbm,
    down_hbm,
    queries,
    forget,
    heads_gain,
    own_hbm,
    mix_hbm,
    out,
    mixer_out,
    gate,
    up,
    down,
    place,
    weigh,
    outgoing,
    features,
    partial,
    paired,
    passed,
    reached,
    result,
    returned,
    mix,
    keys,
    qx,
    top,
    acc,
    s_ref,
    attended,
    gathered,
    load_sem,
    sent,
    go_recv,
    ag_recv,
    rs_recv,
    back_recv,
    az_recv,
    ax_recv,
    bx_recv,
    bz_recv,
    at_recv,
):
    z, x, t = lax.axis_index("ep_0"), lax.axis_index("ep_1"), lax.axis_index("tp")
    me = z * 4 + x
    y, core = t // 2, t % 2
    above = ((y + 1) % 4) * 2 + core
    below = ((y + 3) % 4) * 2 + core
    across = ((y + 2) % 4) * 2 + core
    beside = y * 2 + (1 - core)

    def twin(number):
        return (number // 2) * 2 + 1 - core

    def along(offset):
        peer = (me + offset) % EXPERTS
        return {"ep_0": peer // 4, "ep_1": peer % 4}

    barrier = pltpu.get_barrier_semaphore()
    for offset in range(1, EXPERTS):
        pl.semaphore_signal(barrier, inc=1, device_id=along(offset), device_id_type=MESH)
    for offset in range(1, 8):
        pl.semaphore_signal(
            barrier, inc=1, device_id={"tp": (t + offset) % 8}, device_id_type=MESH
        )
    loads = [
        pltpu.make_async_copy(source, target, load_sem.at[number])
        for number, (source, target) in enumerate(
            (
                (own_hbm, keys.at[me]),
                (gate_hbm, gate),
                (up_hbm, up),
                (down_hbm, down),
                (mix_hbm, mix),
            )
        )
    ]
    for load in loads:
        load.start()

    values = tokens[...].astype(jnp.float32)
    inverse = lax.rsqrt(jnp.mean(values * values, axis=1, keepdims=True) + epsilon)
    columns = pl.ds(pl.multiple_of(t * PART, PART), PART)
    own = (tokens[:, columns].astype(jnp.float32) * inverse * gain[:, columns]).astype(
        jnp.bfloat16
    )
    picks = routes[...]
    raised = jnp.exp(logits[...] - jnp.max(logits[...], axis=0, keepdims=True))
    route_weight = raised / jnp.sum(raised, axis=0, keepdims=True)
    number = lax.broadcasted_iota(jnp.int32, (EXPERTS, TOKENS), 0)
    offset = jnp.where(number % 2 == 1, (number + 1) // 2, (EXPERTS - number // 2) % EXPERTS)
    expert = (me + offset) % EXPERTS
    named = jnp.zeros((EXPERTS, TOKENS), jnp.float32)
    share = jnp.zeros((EXPERTS, TOKENS), jnp.float32)
    for pick in range(4):
        same = picks[pick : pick + 1, :] == expert
        named = named + jnp.where(same, 1.0, 0.0)
        share = share + jnp.where(same, route_weight[pick : pick + 1, :], 0.0)
    before = (
        lax.broadcasted_iota(jnp.int32, (TOKENS, TOKENS), 0)
        < lax.broadcasted_iota(jnp.int32, (TOKENS, TOKENS), 1)
    )
    rank = jnp.dot(
        named.astype(jnp.bfloat16),
        jnp.where(before, 1.0, 0.0).astype(jnp.bfloat16),
        preferred_element_type=jnp.float32,
    )
    slot = jnp.where(named > 0.0, rank, -1.0)
    share_high = share.astype(jnp.bfloat16).astype(jnp.float32)
    share_low = share - share_high
    level = lax.broadcasted_iota(jnp.int32, (SLOTS, TOKENS), 0).astype(jnp.float32)
    for position in range(EXPERTS):
        hit = level == slot[position : position + 1, :]
        rows = slice(position * SLOTS, (position + 1) * SLOTS)
        place[rows, :] = jnp.where(hit, 1.0, 0.0).astype(jnp.bfloat16)
        weigh[0, rows, :] = jnp.where(hit, share_high[position : position + 1, :], 0.0).astype(
            jnp.bfloat16
        )
        weigh[1, rows, :] = jnp.where(hit, share_low[position : position + 1, :], 0.0).astype(
            jnp.bfloat16
        )
    outgoing[...] = jnp.dot(place[...], own, preferred_element_type=jnp.float32).astype(
        jnp.bfloat16
    )
    features[t, 0:SLOTS, :] = outgoing[0:SLOTS, :]
    pl.semaphore_wait(barrier, EXPERTS - 1 + 7)

    def send(source, target, send_sem, recv_sem, device):
        copy = pltpu.make_async_remote_copy(
            src_ref=source,
            dst_ref=target,
            send_sem=send_sem,
            recv_sem=recv_sem,
            device_id=device,
            device_id_type=MESH,
        )
        copy.start()

    def slots(position):
        return pl.ds(position * SLOTS, SLOTS)

    for position in range(1, EXPERTS):
        landing = mirror(position)
        send(
            outgoing.at[slots(position)],
            features.at[t, slots(landing)],
            sent.at[0],
            go_recv.at[landing // PER_CHUNK],
            along(offset_at(position)),
        )

    def rows_of(chunk):
        return pl.ds(chunk * CHUNK, CHUNK)

    def spread(chunk):
        first = SLOTS if chunk == 0 else 0
        landed(
            features.at[t, pl.ds(chunk * CHUNK + first, CHUNK - first)], go_recv.at[chunk]
        )
        block = features.at[t, rows_of(chunk)]
        for kind, target in ((0, above), (1, below), (3, beside)):
            send(block, block, sent.at[1], ag_recv.at[chunk, kind], {"tp": target})

    def forward(chunk):
        for kind, source, target, first in ((0, below, above, 0), (1, above, below, HALF)):
            block = features.at[source, rows_of(chunk)]
            landed(block, ag_recv.at[chunk, kind])
            part = features.at[source, pl.ds(chunk * CHUNK + first, HALF)]
            send(part, part, sent.at[1], ag_recv.at[chunk, 2], {"tp": target})
            send(block, block, sent.at[1], ag_recv.at[chunk, 3], {"tp": beside})

    def complete(chunk):
        block = features.at[across, rows_of(chunk)]
        landed(block, ag_recv.at[chunk, 2])
        send(block, block, sent.at[1], ag_recv.at[chunk, 3], {"tp": beside})

    def multiply(chunk):
        landed(features.at[pl.ds(0, 4), rows_of(chunk)], ag_recv.at[chunk, 3])
        if chunk == 0:
            for load in loads[1:4]:
                load.wait()
        gate_sum = jnp.zeros((CHUNK, PART), jnp.float32)
        up_sum = jnp.zeros((CHUNK, PART), jnp.float32)
        for source in range(8):
            rows = features[source, rows_of(chunk), :]
            depth = slice(source * PART, (source + 1) * PART)
            gate_sum = gate_sum + jnp.dot(rows, gate[depth, :], preferred_element_type=jnp.float32)
            up_sum = up_sum + jnp.dot(rows, up[depth, :], preferred_element_type=jnp.float32)
        gate_cut = jnp.minimum(gate_sum, clamp_limit)
        up_cut = jnp.clip(up_sum, -clamp_limit, clamp_limit)
        hidden = ((up_cut + 1.0) * gate_cut * jax.nn.sigmoid(sigmoid_slope * gate_cut)).astype(
            jnp.bfloat16
        )
        for other in (1, 0):
            for turn in range(4):
                target = ((y + turn) % 4) * 2 + ((1 - core) if other else core)
                partial[chunk, other, turn] = jnp.dot(
                    hidden,
                    down[:, pl.ds(pl.multiple_of(target * PART, PART), PART)],
                    preferred_element_type=jnp.float32,
                ).astype(jnp.bfloat16)
            if other:
                send(
                    partial.at[chunk, 1],
                    paired.at[chunk],
                    sent.at[2],
                    rs_recv.at[chunk, 0],
                    {"tp": beside},
                )

    def added(*values):
        total = values[0].astype(jnp.float32)
        for value in values[1:]:
            total = total + value.astype(jnp.float32)
        return total.astype(jnp.bfloat16)

    def join(chunk):
        landed(paired.at[chunk], rs_recv.at[chunk, 0])
        partial[chunk, 0, 2] = added(partial[chunk, 0, 2], paired[chunk, 2])
        for kind, first, target in ((1, 0, above), (2, HALF, below)):
            send(
                partial.at[chunk, 0, 2, pl.ds(first, HALF)],
                passed.at[chunk, kind - 1],
                sent.at[2],
                rs_recv.at[chunk, kind],
                {"tp": target},
            )
        for turn in (1, 3, 0):
            partial[chunk, 0, turn] = added(partial[chunk, 0, turn], paired[chunk, turn])

    def pass_on(chunk):
        for kind, turn, first, target in ((1, 1, 0, above), (2, 3, HALF, below)):
            landed(passed.at[chunk, kind - 1], rs_recv.at[chunk, kind])
            rows = slice(first, first + HALF)
            partial[chunk, 0, turn, rows] = added(
                partial[chunk, 0, turn, rows], passed[chunk, kind - 1]
            )
            send(
                partial.at[chunk, 0, turn],
                reached.at[chunk, kind - 1],
                sent.at[2],
                rs_recv.at[chunk, 3],
                {"tp": target},
            )

    def finish(chunk):
        landed(reached.at[chunk], rs_recv.at[chunk, 3])
        result[rows_of(chunk), :] = added(
            partial[chunk, 0, 0], reached[chunk, 0], reached[chunk, 1]
        )
        for position in range(chunk * PER_CHUNK, (chunk + 1) * PER_CHUNK):
            if position == 0:
                returned[0:SLOTS, :] = result[0:SLOTS, :]
                continue
            landing = mirror(position)
            send(
                result.at[slots(position)],
                returned.at[slots(landing)],
                sent.at[3],
                back_recv.at[0],
                along(offset_at(position)),
            )

    def plane_of(turn):
        step = (turn + 1) // 2
        return (z + (8 - step if turn % 2 else step)) % PLANES

    def block_of(turn, side):
        return plane_of(turn) * 4 + (x + side) % 4

    a_rows = pl.ds(0, FIRST)
    a_halves = (pl.ds(0, FIRST // 2), pl.ds(FIRST // 2, FIRST // 2))
    b_rows = pl.ds(FIRST, SECOND)
    b_halves = (pl.ds(FIRST, SECOND // 2), pl.ds(FIRST + SECOND // 2, SECOND // 2))
    z_next = ({"ep_0": (z + 1) % PLANES}, {"ep_0": (z + 7) % PLANES})
    x_next = ({"ep_1": (x + 1) % 4}, {"ep_1": (x + 3) % 4})

    def along_x(turn):
        piece = keys.at[block_of(turn, 0), a_rows]
        for way in range(2):
            send(piece, piece, sent.at[4], ax_recv.at[turn, way], x_next[way])

    def keys_start():
        loads[0].wait()
        piece = keys.at[me, a_rows]
        for way in range(2):
            send(piece, piece, sent.at[4], az_recv.at[way, 0], z_next[way])
        rest = keys.at[me, b_rows]
        for way in range(2):
            send(rest, rest, sent.at[4], bx_recv.at[way], x_next[way])
        along_x(0)

    def turn_at(step, way):
        return 7 if step == 4 else 2 * step - 1 + way

    def a_z(step):
        for way in range(2):
            block = block_of(turn_at(step, way), 0)
            rows = a_rows if step < 4 else a_halves[way]
            landed(keys.at[block, rows], az_recv.at[way, step - 1])
            if step < 4:
                piece = keys.at[block, a_rows if step < 3 else a_halves[way]]
                send(piece, piece, sent.at[4], az_recv.at[way, step], z_next[way])
                along_x(turn_at(step, way))
        if step == 4:
            along_x(7)

    def a_x(turn):
        for way, side in ((0, 3), (1, 1)):
            block = block_of(turn, side)
            landed(keys.at[block, a_rows], ax_recv.at[turn, way])
            piece = keys.at[block, a_halves[way]]
            send(piece, piece, sent.at[4], ax_recv.at[turn, 2], x_next[way])

    def a_done(turn):
        landed(keys.at[block_of(turn, 2), a_rows], ax_recv.at[turn, 2])

    def b_x():
        for way, side in ((0, 3), (1, 1)):
            block = block_of(0, side)
            landed(keys.at[block, b_rows], bx_recv.at[way])
            piece = keys.at[block, b_halves[way]]
            send(piece, piece, sent.at[4], bx_recv.at[2], x_next[way])

    def b_row():
        landed(keys.at[block_of(0, 2), b_rows], bx_recv.at[2])
        pieces = keys.at[pl.ds(z * 4, 4), b_rows]
        for way in range(2):
            send(pieces, pieces, sent.at[4], bz_recv.at[way, 0], z_next[way])

    def b_z(step):
        for way in range(2):
            blocks = pl.ds(plane_of(turn_at(step, way)) * 4, 4)
            rows = b_rows if step < 4 else b_halves[way]
            landed(keys.at[blocks, rows], bz_recv.at[way, step - 1])
            if step < 4:
                pieces = keys.at[blocks, b_rows if step < 3 else b_halves[way]]
                send(pieces, pieces, sent.at[4], bz_recv.at[way, step], z_next[way])

    start = forget[:, pl.ds(pl.multiple_of(me * ROWS, ROWS), 128)][:, 0:1]

    def key_rows(block):
        gate_rows = pl.ds(pl.multiple_of(block * ROWS, ROWS), ROWS)
        return key_operand(keys[block], forget[:, gate_rows] - start)

    def own_block():
        query_operand(queries[...], qx)
        lanes = key_rows(me)
        values = value_operand(keys[me])
        for tile in range(ASKED // TILE):
            cut = slice(tile * TILE, (tile + 1) * TILE)
            scores = jnp.dot(lanes, qx[:, cut], preferred_element_type=jnp.float32)
            key_at = lax.broadcasted_iota(jnp.int32, (ROWS, TILE), 0)
            query_at = lax.broadcasted_iota(jnp.int32, (ROWS, TILE), 1) + (tile * TILE) % ROWS
            scores = jnp.where(key_at <= query_at, scores, -jnp.inf)
            new = jnp.max(scores, axis=0, keepdims=True)
            weights = jnp.exp(scores - new).astype(jnp.bfloat16)
            acc[:, cut] = jnp.dot(values, weights, preferred_element_type=jnp.float32)
            top[:, cut] = new

    def take(block, after, slot):
        lanes = key_rows(after)
        values = value_operand(keys[block])
        for tile in range(ASKED // TILE):
            cut = slice(tile * TILE, (tile + 1) * TILE)
            s_ref[1 - slot, :, cut] = jnp.dot(
                lanes, qx[:, cut], preferred_element_type=jnp.float32
            )
            scores = s_ref[slot, :, cut]
            old = top[:, cut]
            new = jnp.maximum(old, jnp.max(scores, axis=0, keepdims=True))
            weights = jnp.exp(scores - new).astype(jnp.bfloat16)
            acc[:, cut] = acc[:, cut] * jnp.exp(old - new) + jnp.dot(
                values, weights, preferred_element_type=jnp.float32
            )
            top[:, cut] = new

    def attend(first, count):
        @pl.when(count > 0)
        def _():
            lanes = key_rows(first)
            for tile in range(ASKED // TILE):
                cut = slice(tile * TILE, (tile + 1) * TILE)
                s_ref[0, :, cut] = jnp.dot(
                    lanes, qx[:, cut], preferred_element_type=jnp.float32
                )
            last = first + count - 1

            def pair(step, _):
                block = first + 2 * step
                take(block, jnp.minimum(block + 1, last), 0)

                @pl.when(block + 1 <= last)
                def _():
                    take(block + 1, jnp.minimum(block + 2, last), 1)

                return 0

            lax.fori_loop(0, (count + 1) // 2, pair, 0)

    before_rounds = (
        (keys_start,), (own_block,), (spread, 0), (spread, 1), (forward, 0), (b_x,), (a_x, 0),
        (spread, 2), (forward, 1), (complete, 0), (a_z, 1), (b_row,), (spread, 3), (a_done, 0),
        (a_x, 1), (a_x, 2), (forward, 2), (complete, 1),
    )
    rounds = (
        (),
        ((a_z, 2), (b_z, 1), (multiply, 0), (a_done, 1), (a_done, 2)),
        (
            (join, 0), (forward, 3), (complete, 2), (a_x, 3), (a_x, 4), (a_z, 3), (multiply, 1),
        ),
        (
            (join, 1), (pass_on, 0), (b_z, 2), (a_x, 5), (a_x, 6), (complete, 3), (a_z, 4),
            (multiply, 2), (a_done, 3),
        ),
        ((pass_on, 1), (finish, 0), (join, 2), (multiply, 3), (a_x, 7), (a_done, 4)),
        ((b_z, 3), (join, 3), (pass_on, 2), (finish, 1), (a_done, 5)),
        ((pass_on, 3), (finish, 2), (a_done, 6)),
        ((b_z, 4), (finish, 3), (a_done, 7)),
    )

    for step, *at in before_rounds:
        step(*at)

    def one_round(turn, _):
        for number, events in enumerate(rounds):
            if events:

                @pl.when(turn == number)
                def _(events=events):
                    for step, *at in events:
                        step(*at)

        odd = turn % 2
        step = (turn + 1) // 2
        plane = jnp.where(odd == 1, z - step, z + step - jnp.where(turn > 0, PLANES, 0))
        count = jnp.where(turn == 0, x, jnp.where(plane >= 0, 4, 0))
        attend(jnp.maximum(plane, 0) * 4, count)
        return 0

    lax.fori_loop(0, PLANES, one_round, 0)

    total = acc[...]
    heads = total[0:HEAD] / total[HEAD : HEAD + 1]
    both = jnp.concatenate([heads[:, 0:ROWS], heads[:, ROWS:ASKED]], axis=0)
    attended[...] = both.T.astype(jnp.bfloat16)
    for offset in range(1, 8):
        peer = (t + offset) % 8
        send(
            attended.at[pl.ds(pl.multiple_of(peer * SHARE, SHARE), SHARE)],
            gathered.at[t],
            sent.at[5],
            at_recv.at[0],
            {"tp": peer},
        )
    gathered[t] = attended[pl.ds(pl.multiple_of(t * SHARE, SHARE), SHARE), :]

    loads[4].wait()
    landed(gathered.at[pl.ds(0, 7)], at_recv.at[0])
    rows = jnp.concatenate([gathered[source] for source in range(8)], axis=1).astype(jnp.float32)
    inverse = lax.rsqrt(jnp.mean(rows * rows, axis=1, keepdims=True) + epsilon)
    normed = (rows * inverse * heads_gain[...]).astype(jnp.bfloat16)
    mixer_out[...] = jnp.dot(normed, mix[...], preferred_element_type=jnp.float32).astype(
        jnp.bfloat16
    )

    landed(returned.at[pl.ds(SLOTS, ALL_SLOTS - SLOTS)], back_recv.at[0])
    turned = (((0,), (0,)), ((), ()))
    out[...] = (
        lax.dot_general(weigh[0], returned[...], turned, preferred_element_type=jnp.float32)
        + lax.dot_general(weigh[1], returned[...], turned, preferred_element_type=jnp.float32)
    ).astype(jnp.bfloat16)

    rest = pl.ds(0, ALL_SLOTS - SLOTS)
    landed(outgoing.at[rest], sent.at[0])
    landed(features.at[pl.ds(0, 7)], sent.at[1])
    landed(features.at[pl.ds(0, 7)], sent.at[2])
    landed(result.at[rest], sent.at[3])
    landed(keys.at[pl.ds(0, EXPERTS - 1)], sent.at[4])
    landed(gathered.at[pl.ds(0, 7)], sent.at[5])


def body(
    queries,
    keys_values,
    forget_cache,
    heads_gain,
    output_weight,
    expert_tokens,
    expert_gain,
    routes,
    route_logits,
    gate_weight,
    up_weight,
    down_weight,
):
    vmem = pl.BlockSpec(memory_space=pltpu.VMEM)
    anywhere = pl.BlockSpec(memory_space=pl.ANY)
    half = jnp.bfloat16
    dma = pltpu.SemaphoreType.DMA
    moe_out, mixer_out = pl.pallas_call(
        kernel,
        out_shape=(
            jax.ShapeDtypeStruct((TOKENS, PART), half),
            jax.ShapeDtypeStruct((SHARE, WIDTH), half),
        ),
        in_specs=[vmem] * 4 + [anywhere] * 3 + [vmem] * 3 + [anywhere] * 2,
        out_specs=(vmem, vmem),
        scratch_shapes=[
            pltpu.VMEM((WIDTH, PART), half),
            pltpu.VMEM((WIDTH, PART), half),
            pltpu.VMEM((PART, WIDTH), half),
            pltpu.VMEM((ALL_SLOTS, TOKENS), half),
            pltpu.VMEM((2, ALL_SLOTS, TOKENS), half),
            pltpu.VMEM((ALL_SLOTS, PART), half),
            pltpu.VMEM((8, ALL_SLOTS, PART), half),
            pltpu.VMEM((CHUNKS, 2, 4, CHUNK, PART), half),
            pltpu.VMEM((CHUNKS, 4, CHUNK, PART), half),
            pltpu.VMEM((CHUNKS, 2, HALF, PART), half),
            pltpu.VMEM((CHUNKS, 2, CHUNK, PART), half),
            pltpu.VMEM((ALL_SLOTS, PART), half),
            pltpu.VMEM((ALL_SLOTS, PART), half),
            pltpu.VMEM((16 * HEAD, WIDTH), half),
            pltpu.VMEM((4 * PLANES, ROWS, 2 * HEAD), half),
            pltpu.VMEM((2 * HEAD, ASKED), half),
            pltpu.VMEM((1, ASKED), jnp.float32),
            pltpu.VMEM((HEAD + 16, ASKED), jnp.float32),
            pltpu.VMEM((2, ROWS, ASKED), jnp.float32),
            pltpu.VMEM((ROWS, 2 * HEAD), half),
            pltpu.VMEM((8, SHARE, 2 * HEAD), half),
            dma((5,)),
            dma((6,)),
            dma((CHUNKS,)),
            dma((CHUNKS, 4)),
            dma((CHUNKS, 4)),
            dma((1,)),
            dma((2, 4)),
            dma((PLANES, 3)),
            dma((3,)),
            dma((2, 4)),
            dma((1,)),
        ],
        compiler_params=pltpu.CompilerParams(
            collective_id=0, has_side_effects=True, vmem_limit_bytes=60 * 2**20
        ),
    )(
        expert_tokens,
        expert_gain.reshape(1, -1),
        routes.T,
        route_logits.T,
        gate_weight[0],
        up_weight[0],
        down_weight[0],
        queries,
        forget_cache,
        heads_gain.reshape(1, -1),
        keys_values,
        output_weight,
    )
    return (mixer_out, moe_out)


def solution(mesh):
    torus = Mesh(mesh.devices.reshape(8, 4, mesh.shape["tp"]), ("ep_0", "ep_1", "tp"))
    return jax.shard_map(
        body,
        mesh=torus,
        in_specs=(
            P(EP, "tp"),
            P(EP, "tp"),
            P("tp", None),
            P(),
            P(),
            P(EP, None),
            P(),
            P(EP, None),
            P(EP, None),
            P(EP, None, "tp"),
            P(EP, None, "tp"),
            P(EP, "tp", None),
        ),
        out_specs=(P(EP_TP, None), P(EP, "tp")),
        check_vma=False,
    )
```
